32 devices in a mesh: gr: 2 (over core), fs: 8 (over z, y), tp: 2 (over x).
Axes of the slice: x: 2, y: 2, z: 4, core: 2. Of those that a mesh axis runs over, the one named last changes fastest.
Arguments:
- tokens: bfloat16 [3072, 2048], P(('gr', 'fs')), may hold values from -6 to 6
- routes: int32 [3072, 8], P(('gr', 'fs')), may hold values from 0 to 15, all different within a row; in each aligned block of 192 rows (0 to 191, 192 to 383, ...) at most 144 rows name the same one
- route_weight: float32 [3072, 8], P(('gr', 'fs')), may hold values from 0.05 to 0.6
- norm_gain: float32 [2048], replicated, may hold values from 0.1 to 1.9
- gate_experts: float32 [2, 8, 512, 2048], P('gr', None, 'fs', 'tp'), may hold values from -0.125 to 0.125
- up_experts: float32 [2, 8, 512, 2048], P('gr', None, 'fs', 'tp'), may hold values from -0.125 to 0.125
- down_experts: float32 [2, 8, 512, 2048], P('gr', None, 'fs', 'tp'), may hold values from -0.25 to 0.25
- gate_shared: float32 [2048, 512], P('fs', 'tp'), may hold values from -0.125 to 0.125
- up_shared: float32 [2048, 512], P('fs', 'tp'), may hold values from -0.125 to 0.125
- down_shared: float32 [512, 2048], P('fs', 'tp'), may hold values from -0.25 to 0.25
Outputs:
- mixed: bfloat16 [3072, 2048], P(('gr', 'fs'), 'tp')
- gate_served: bfloat16 [2, 8, 512, 2048], P(None, 'fs', 'tp')
- up_served: bfloat16 [2, 8, 512, 2048], P(None, 'fs', 'tp')
- down_served: bfloat16 [2, 8, 512, 2048], P(None, 'fs', None, 'tp')
- gate_shared_served: bfloat16 [2048, 512], P(None, 'tp')
- up_shared_served: bfloat16 [2048, 512], P(None, 'tp')
- down_shared_served: bfloat16 [512, 2048], P(None, 'tp')
The draws below stay inside these ranges and needn't reach their ends.
Inputs may be any that keep to these rules, and one draw needn't show every extreme that they name: `routes`: each row names 8 different experts; within the 192 rows of one device no expert is named by more than 144 rows, and some expert reaches 144.
All inputs are finite; a program needn't handle non-finite values.
Results may differ from the reference program's by a relative error of at most 0.0084.
Values may be sent and summed in bfloat16 or wider, within the bound.
A program may use at most 128 MiB of HBM per device.

```python
import math
import jax
import jax.numpy as jnp
import numpy as np
from jax import lax

D = 2048
DE = 512
DS = 512
TOP_K = 8
EXP_HALF = 1
TOK_DEV = 192
EXPERTS = 16
CAP = 144
TOKENS = 3072
N_GR = 2
N_FS = 8


def shard_levels(own_key, shape, pieces, low, largest):
    gain = 1.0
    for dim, shards_of in pieces:
        heights = jax.random.uniform(jax.random.fold_in(jax.random.fold_in(own_key, 6), dim), (shards_of,), jnp.float32, low / len(pieces), largest / len(pieces))
        gain = gain * jnp.repeat(jnp.exp(heights), shape[dim] // shards_of).reshape((-1,) + (1,) * (len(shape) - 1 - dim))
    return gain


def shared_out(stream_key, own, number, rows, number_of, top, most, slope):
    order = jax.random.permutation(stream_key, number_of)
    packed, ordinary = portions_of(number_of, rows * top, most, slope, True), portions_of(number_of, rows * top, most, slope, False)
    places = jnp.arange(number_of)

    def named(lengths, turn):
        used = int((lengths > 0).sum())
        fixed = max(1, used // 4)
        moved = fixed + (places - fixed + turn * (used - fixed)) % max(1, number_of - fixed)
        return jnp.zeros((number_of,), jnp.int32).at[order[jnp.where(places < fixed, places, moved)]].set(jnp.asarray(lengths, jnp.int32))

    lengths = jnp.where(number % 4 == 0, named(packed, number // 4), named(ordinary, number - number // 4 - 1))
    mixed = jax.random.permutation(jax.random.fold_in(own, 3), number_of)
    source_of, sink = mixed[0:number_of // 2 * 2:2], mixed[1:number_of // 2 * 2:2]
    margin = jnp.minimum(lengths[source_of] - 1, most - lengths[sink]) // 2
    margin = jnp.where((source_of == order[0]) | (sink == order[0]) | (lengths[sink] == 0), 0, jnp.maximum(margin, 0))
    moved = jax.random.randint(jax.random.fold_in(own, 4), (number_of // 2,), 0, 1 << 20) % (margin + 1)
    lengths = lengths.at[source_of].add(-moved).at[sink].add(moved)
    items = jnp.searchsorted(jnp.cumsum(lengths), jnp.arange(rows * top), side="right").astype(jnp.int32)
    table = items.reshape(top, rows).T
    table = table[jax.random.permutation(jax.random.fold_in(own, 1), rows)]
    turn = jax.random.randint(jax.random.fold_in(own, 2), (rows, 1), 0, top)
    return jnp.take_along_axis(table, (jnp.arange(top)[None, :] + turn) % top, axis=1)


def portions_of(amount, total, most, skew, full):
    weights = [(1 << 20) // math.isqrt(standing ** skew) + 1 for standing in range(1, amount + 1)]
    largest = most if full else min(most, max(-(-total // amount), total * weights[0] // sum(weights)))
    least = 1 if total - largest >= amount - 1 else 0
    given, surplus = [largest] + [least] * (amount - 1), total - largest - least * (amount - 1)
    while surplus > 0:
        candidates = [i for i in range(1, amount) if given[i] < largest] or [i for i in range(1, amount) if given[i] < most]
        mass, remaining = sum([weights[i] for i in candidates]), surplus
        for i in candidates:
            extra = min(most - given[i], max(1, remaining * weights[i] // mass), surplus)
            given[i] = given[i] + extra
            surplus = surplus - extra
    return np.array(given)


def normal_values(rng, dims, scale, most, pieces=(), kind=jnp.bfloat16):
    entries = scale * jax.random.normal(rng, dims, jnp.float32)
    if pieces:
        entries = entries * shard_levels(rng, dims, pieces, -0.22, 0.18)
    return jnp.clip(entries, -most, most).astype(kind)


def setup_inputs(seed: int = 0) -> dict:
    seeds = jax.random.split(jax.random.key(seed), 11)
    tokens = normal_values(seeds[0], (TOKENS, D), 1.0, 6.0, ((0, 16),))
    routes_keys = jax.random.split(jax.random.fold_in(seeds[1], 1), TOKENS // TOK_DEV)
    routes_turns = jax.random.permutation(jax.random.fold_in(seeds[1], 3), TOKENS // TOK_DEV)
    routes = jax.vmap(lambda own, number: shared_out(jax.random.fold_in(seeds[1], 2), own, number, TOK_DEV, EXPERTS, TOP_K, CAP, 1))(routes_keys, routes_turns).reshape((TOKENS, TOP_K))
    route_weight = jnp.clip(jnp.exp(math.log(0.6) - 2.4849067 * jax.random.uniform(seeds[2], (TOKENS, TOP_K), jnp.float32) ** shard_levels(seeds[2], (TOKENS, TOP_K), ((0, 16),), -0.2, 0.2)), 0.05, 0.6)
    norm_gain = jnp.clip(1.0 + 0.18 * jax.random.normal(seeds[3], (D,), jnp.float32), 0.1, 1.9)
    gate_experts = normal_values(seeds[4], (N_GR, EXP_HALF * N_FS, DE, D), D ** -0.5, 0.125, ((0, 2), (2, 8), (3, 2)), jnp.float32)
    up_experts = normal_values(seeds[5], (N_GR, EXP_HALF * N_FS, DE, D), D ** -0.5, 0.125, ((0, 2), (2, 8), (3, 2)), jnp.float32)
    down_experts = normal_values(seeds[6], (N_GR, EXP_HALF * N_FS, DE, D), DE ** -0.5, 0.25, ((0, 2), (2, 8), (3, 2)), jnp.float32)
    gate_shared = normal_values(seeds[7], (D, DS), D ** -0.5, 0.125, ((0, 8), (1, 2)), jnp.float32)
    up_shared = normal_values(seeds[8], (D, DS), D ** -0.5, 0.125, ((0, 8), (1, 2)), jnp.float32)
    down_shared = normal_values(seeds[9], (DS, D), DS ** -0.5, 0.25, ((0, 8), (1, 2)), jnp.float32)
    return dict(tokens=tokens, routes=routes, route_weight=route_weight, norm_gain=norm_gain, gate_experts=gate_experts, up_experts=up_experts, down_experts=down_experts, gate_shared=gate_shared, up_shared=up_shared, down_shared=down_shared)


EPS = 1e-06

def reference(tokens, routes, route_weight, norm_gain, gate_experts, up_experts, down_experts, gate_shared, up_shared, down_shared):
    bf = jnp.bfloat16
    f32 = jnp.float32
    gate_served = (gate_experts * norm_gain[None, None, None, :]).astype(bf)
    up_served = (up_experts * norm_gain[None, None, None, :]).astype(bf)
    down_served = down_experts.astype(bf)
    gate_sh = (gate_shared * norm_gain[:, None]).astype(bf)
    up_sh = (up_shared * norm_gain[:, None]).astype(bf)
    down_sh = down_shared.astype(bf)
    values = tokens.astype(f32)
    normed = (values * lax.rsqrt(lax.optimization_barrier(jnp.mean(values * values, axis=-1, keepdims=True)) + EPS)).astype(bf)
    count = EXPERTS
    slots_all = CAP * N_GR * N_FS
    flat_e = routes.reshape(-1).astype(jnp.int32)
    assigned = flat_e.shape[0]
    onehot = (flat_e[:, None] == jnp.arange(count, dtype=jnp.int32)[None, :]).astype(jnp.int32)
    ranks = lax.optimization_barrier(jnp.sum(jnp.cumsum(onehot, axis=0) * onehot, axis=1)) - 1
    position = (flat_e * slots_all + ranks).astype(jnp.int32)
    token_of = (jnp.arange(assigned, dtype=jnp.int32) // TOP_K).astype(jnp.int32)
    table = jnp.full((count * slots_all,), TOKENS, jnp.int32).at[position].set(token_of)
    padded = jnp.concatenate([normed, jnp.zeros((1, D), bf)], axis=0)

    def one_expert(args):
        index, w_gate, w_up, w_down = args
        rows = padded[index]
        gate = jnp.dot(rows, w_gate.T, preferred_element_type=f32)
        upper = jnp.dot(rows, w_up.T, preferred_element_type=f32)
        hidden = (jax.nn.silu(gate) * upper).astype(bf)
        return jnp.dot(hidden, w_down, preferred_element_type=f32).astype(bf)
    outputs = lax.map(one_expert, (table.reshape(count, slots_all), gate_served.reshape(count, DE, D), up_served.reshape(count, DE, D), down_served.reshape(count, DE, D)))
    picked = outputs.reshape(count * slots_all, D)[position].reshape(TOKENS, TOP_K, D)
    routed = lax.optimization_barrier(jnp.sum(picked.astype(f32) * route_weight[:, :, None], axis=1))
    shared_hidden = (jax.nn.silu(jnp.dot(normed, gate_sh, preferred_element_type=f32)) * jnp.dot(normed, up_sh, preferred_element_type=f32)).astype(bf)
    shared = jnp.dot(shared_hidden, down_sh, preferred_element_type=f32)
    mixed = (routed + shared).astype(bf)
    return (mixed, gate_served, up_served, down_served, gate_sh, up_sh, down_sh)
```

```python
import functools

import jax
import jax.numpy as jnp
from jax import lax
from jax.experimental import pallas as pl
from jax.experimental.pallas import tpu as pltpu
from jax.sharding import PartitionSpec as P

EPS = 1e-06
MESH = pl.DeviceIdType.MESH
BF = jnp.bfloat16
F32 = jnp.float32


def whole(cfg, rows_in, local_in, gate_l, up_l, down_l, gs_l, us_l, ds_l,
          mixed_o, gate_o, up_o, down_o, gs_o, us_o, ds_o,
          X, W, H, GS, US, DS, SH, SO, PS, YR, S, ZS, ZR, FS, FR,
          b_send, b_recv, b_own, x_send, x_recv, p_send, p_recv,
          c_zs, c_zr, c_ys, c_yr, c_own, g_send, g_recv,
          sh_send, sh_recv, y_send, y_recv, z_send, z_recv, f_send, f_recv, o_sem):
    n_gr, n_fs, n_tp = cfg.dims
    inner, nz, R, NT, CT = cfg.inner, cfg.nz, cfg.R, cfg.NT, cfg.CT
    gr, fs, tp = lax.axis_index("gr"), lax.axis_index("fs"), lax.axis_index("tp")
    z, y = fs // inner, fs % inner
    rows, cols = gate_l.shape[1], gate_l.shape[2]
    width = cols * n_tp
    depth = rows * n_fs
    units = depth // n_tp
    locs = (gate_l, up_l, down_l)

    def ds(start, size):
        if isinstance(start, int):
            return pl.ds(start, size)
        return pl.ds(pl.multiple_of(start * 1, size), size)

    def remote(src, dst, s, r, to):
        return pltpu.make_async_remote_copy(
            src_ref=src, dst_ref=dst, send_sem=s, recv_sem=r, device_id=to, device_id_type=MESH)

    barrier = pltpu.get_barrier_semaphore()

    def greet(d, c):
        pl.semaphore_signal(barrier, inc=1, device_id=(gr, (fs + d) % n_fs, tp), device_id_type=MESH)
        return c
    lax.fori_loop(1, n_fs, greet, 0)
    for q in range(1, n_tp):
        pl.semaphore_signal(barrier, inc=1, device_id=(gr, fs, (tp + q) % n_tp), device_id_type=MESH)
    for p in range(1, n_gr):
        pl.semaphore_signal(barrier, inc=1, device_id=((gr + p) % n_gr, fs, tp), device_id_type=MESH)
    pl.semaphore_wait(barrier, n_fs - 1 + n_tp - 1 + n_gr - 1)

    def block(m, s, t):
        return W.at[m, gr, ds(s * rows, rows), ds(t * cols, cols)]

    def region(m, g, t):
        return W.at[m, g, :, ds(t * cols, cols)]

    def to_expert(m, k):
        return remote(locs[m].at[k], block(m, fs, tp), b_send.at[m], b_recv.at[m, fs], (gr, k, tp))

    def own_block(m):
        return pltpu.make_async_copy(locs[m].at[fs], block(m, fs, tp), b_own.at[m])

    def each_other(act):
        def step(d, c):
            pl.when(fs + d < n_fs)(lambda: act(fs + d))
            pl.when(fs - d >= 0)(lambda: act(fs - d))
            return c
        lax.fori_loop(1, n_fs, step, 0)

    def across(m, src, s):
        for q in range(1, n_tp):
            remote(src, block(m, s, tp), x_send.at[m, q - 1], x_recv.at[m, q - 1],
                   (gr, fs, (tp + q) % n_tp)).start()

    def send_matrix(m):
        each_other(lambda k: to_expert(m, k).start())
        own_block(m).start()
        across(m, locs[m].at[fs], fs)

    def landed(m, s):
        part = block(m, s, tp)
        remote(part, part, b_recv.at[m, s], b_recv.at[m, s], (gr, s, tp)).wait_recv()
        across(m, part, s)

    def partner(m, g, q, p):
        part = region(m, g, (tp + n_tp - q) % n_tp)
        return remote(part, part, p_send.at[m, q, p - 1], p_recv.at[m, q, p - 1],
                      ((gr + p) % n_gr, fs, tp))

    def share(m, q):
        for p in range(1, n_gr):
            partner(m, gr, q, p).start()

    def shared_landed(m, q):
        for p in range(1, n_gr):
            partner(m, (gr + n_gr - p) % n_gr, q, p).wait_recv()

    def x_landed(m, q):
        part = region(m, gr, (tp + n_tp - q) % n_tp)
        remote(part, part, x_send.at[m, q - 1], x_recv.at[m, q - 1],
               (gr, fs, (tp + q) % n_tp)).wait_recv()

    big = ((rows_in, lambda zz, yr: X.at[ds((yr * nz + zz) * R, R), :], 1),)

    def shared_item(src, dst, parts):
        size = src.shape[0] // parts

        def place(zz, yr):
            f = zz * inner + (y + yr) % inner
            if parts == 1:
                return dst.at[ds(f * size, size), :]
            return dst.at[ds((f * parts + gr) * size, size), :]
        own = src if parts == 1 else src.at[ds(gr * size, size), :]
        return (own, place, parts)
    small = tuple(shared_item(s, d, p) for s, d, p in zip((gs_l, us_l, ds_l), (GS, US, DS), cfg.parts))
    items = big + small

    def at(way, d):
        return z - d if way == 0 else z + d

    def z_copy(m, way, d):
        own, place, _ = items[m]
        dst = place(at(way, d), 0)
        return remote(own if d == 0 else dst, dst, c_zs.at[m, way, d], c_zr.at[m, way, d],
                      (gr, (z + 1 if way == 0 else z - 1) * inner + y, tp))

    def y_slot(d, way):
        return d + way * (nz - 1) if d else 0

    def y_copy(m, q, way, d):
        own, place, parts = items[m]
        zz = at(way, d)
        src = own if d == 0 else place(zz, 0)
        dst = place(zz, inner - q) if m == 0 else place(zz, 0)
        i = y_slot(d, way)
        return remote(src, dst, c_ys.at[m, q - 1, i], c_yr.at[m, q - 1, i],
                      (gr, z * inner + (y + q) % inner, tp))

    def pass_partner(m, part):
        if items[m][2] > 1:
            for p in range(1, n_gr):
                remote(part, part, g_send.at[m, p - 1], g_recv.at[m, p - 1],
                       ((gr + p) % n_gr, fs, tp)).start()

    def next_there(way):
        return (z < nz - 1) if way == 0 else (z > 0)

    def there(d, way):
        return (z - d >= 0) if way == 0 else (z + d < nz)

    def gather_start(m):
        own, place, parts = items[m]
        for way in (0, 1):
            pl.when(next_there(way))(lambda way=way: z_copy(m, way, 0).start())
        for q in range(1, inner):
            y_copy(m, q, 0, 0).start()
        pltpu.make_async_copy(own, place(z, 0), c_own.at[m]).start()

    def gather_own(m):
        own, place, parts = items[m]
        pltpu.make_async_copy(own, place(z, 0), c_own.at[m]).wait()
        pass_partner(m, place(z, 0))

    def gather_pass(m, d):
        for way in (0, 1):
            def act(way=way):
                part = items[m][1](at(way, d), 0)
                remote(part, part, c_zs.at[m, way, d - 1], c_zr.at[m, way, d - 1],
                       (gr, (z + 1 if way == 0 else z - 1) * inner + y, tp)).wait_recv()
                if d < nz - 1:
                    pl.when(next_there(way))(lambda: z_copy(m, way, d).start())
                for q in range(1, inner):
                    y_copy(m, q, way, d).start()
                pass_partner(m, part)
            pl.when(there(d, way))(act)

    places = [(0, 0)] + [(d, way) for d in range(1, nz) for way in (0, 1)]

    def gather_y(m):
        for d, way in places:
            def act(d=d, way=way):
                for q in range(1, inner):
                    part = items[m][1](at(way, d), inner - q)
                    i = y_slot(d, way)
                    remote(part, part, c_ys.at[m, q - 1, i], c_yr.at[m, q - 1, i],
                           (gr, z * inner + (y + q) % inner, tp)).wait_recv()
                    pass_partner(m, part)
            if d == 0:
                act()
            else:
                pl.when(there(d, way))(act)

    def gather_sent(m):
        for d, way in places:
            def act(d=d, way=way):
                for w in ((0, 1) if d == 0 else (way,)):
                    if d < nz - 1:
                        pl.when(next_there(w))(lambda w=w: z_copy(m, w, d).wait_send())
                for q in range(1, inner):
                    y_copy(m, q, way, d).wait_send()
            if d == 0:
                act()
            else:
                pl.when(there(d, way))(act)

    def partner_gathered(m, way):
        dst = (X, GS, US, DS)[m]
        if items[m][2] > 1:
            part = dst.at[pl.ds(0, dst.shape[0] // items[m][2]), :]
            for p in range(1, n_gr):
                c = remote(part, part, g_send.at[m, p - 1], g_recv.at[m, p - 1],
                           ((gr + p) % n_gr, fs, tp))
                if way:
                    c.wait_send()
                else:
                    c.wait_recv()

    gather_start(0)
    send_matrix(0)
    if nz > 1:
        gather_pass(0, 1)
    send_matrix(1)
    if nz > 2:
        gather_pass(0, 2)
    for m in (1, 2, 3):
        gather_start(m)
    send_matrix(2)
    for d in range(3, nz):
        gather_pass(0, d)
    for m in (1, 2, 3):
        gather_own(m)
    for m in (0, 1):
        each_other(lambda s: landed(m, s))
        own_block(m).wait()
        share(m, 0)
        if m:
            for q in range(1, n_tp):
                x_landed(0, q)
                share(0, q)
    for q in range(1, n_tp):
        x_landed(1, q)
        share(1, q)
    pltpu.make_async_copy(rows_in, items[0][1](z, 0), c_own.at[0]).wait()
    gather_y(0)

    outs = (gate_o, up_o)

    def out_wide(m, g):
        return pltpu.make_async_copy(W.at[m, g, ds(tp * units, units), :], outs[m].at[g, 0], o_sem.at[m, g])

    def out_tall(g):
        return pltpu.make_async_copy(region(2, g, tp), down_o.at[g, 0], o_sem.at[2, g])

    NB = cfg.NB
    per = depth // NB
    chunks = n_gr * per
    count = n_gr * n_fs
    lanes = lax.broadcasted_iota(jnp.int32, (n_fs * R, 128), 1)

    def chunk(i, c):
        gg = (gr + i // per) % n_gr
        n = i % per

        @pl.when(i % per == 0)
        def _():
            @pl.when(i > 0)
            def _():
                for m in (0, 1):
                    for q in range(n_tp):
                        for p in range(1, n_gr):
                            pl.when(i // per == n_gr - p)(
                                lambda m=m, q=q, p=p: partner(m, (gr + n_gr - p) % n_gr, q, p).wait_recv())
            for m in (0, 1):
                out_wide(m, gg).start()
        x = X[:, pl.ds(0, width)]
        expert = gg * n_fs + fs
        weight = jnp.zeros((n_fs * R, 1), F32)
        for k in range(cfg.extra // 128):
            tail = X[:, pl.ds(width + k * 128, 128)].astype(F32)
            pick = (lanes + k * 128 == expert) | (lanes + k * 128 == count + expert)
            weight = weight + jnp.sum(jnp.where(pick, tail, 0.0), axis=1, keepdims=True)
        dn = (((1,), (1,)), ((), ()))
        gate = lax.dot_general(x, W[0, gg, ds(n * NB, NB), :], dn, preferred_element_type=F32)
        upper = lax.dot_general(x, W[1, gg, ds(n * NB, NB), :], dn, preferred_element_type=F32)
        H[:, ds((gg * per + n) * NB, NB)] = (gate / (1.0 + jnp.exp(-gate)) * upper * weight).astype(BF)
        each = -(-(n_fs - 1) // chunks)

        def some(e, c):
            d = 1 + i * each + e

            @pl.when(d < n_fs)
            def _():
                pl.when(fs + d < n_fs)(lambda: landed(2, fs + d))
                pl.when(fs - d >= 0)(lambda: landed(2, fs - d))
            return c
        lax.fori_loop(0, each, some, 0)
        return c
    lax.fori_loop(0, chunks, chunk, 0)
    own_block(2).wait()
    share(2, 0)

    for d in range(1, nz):
        for m in (1, 2, 3):
            gather_pass(m, d)
    for m in (1, 2, 3):
        gather_y(m)
        partner_gathered(m, 0)
    sg = jnp.dot(local_in[...], GS[...], preferred_element_type=F32)
    su = jnp.dot(local_in[...], US[...], preferred_element_type=F32)
    SH[pl.ds(tp, 1)] = (sg / (1.0 + jnp.exp(-sg)) * su).astype(BF)[None]
    shared_outs = [pltpu.make_async_copy(a, b, o_sem.at[3 + i, 0])
                   for i, (a, b) in enumerate(((GS, gs_o), (US, us_o), (DS, ds_o)))]
    for c in shared_outs:
        c.start()
    for q in range(1, n_tp):
        x_landed(2, q)
        share(2, q)

    def sh_copy(q):
        return remote(SH.at[tp], SH.at[tp], sh_send.at[q - 1], sh_recv.at[q - 1],
                      (gr, fs, (tp + q) % n_tp))
    for q in range(1, n_tp):
        sh_copy(q).start()
    shared_landed(2, 0)

    tiles = NT // n_tp
    half = nz * R

    def col(i):
        return (tp * tiles + i) % NT

    def y_out(i, r):
        return remote(PS.at[i, r - 1], YR.at[i, r - 1], y_send.at[i, r - 1], y_recv.at[i, r - 1],
                      (gr, z * inner + (y + r) % inner, tp))

    def produce(i, c):
        @pl.when(i == tiles)
        def _():
            for q in range(1, n_tp):
                shared_landed(2, q)
        part = jnp.zeros((n_fs * R, CT), F32)
        for g in range(n_gr):
            part = part + jnp.dot(H[:, pl.ds(g * depth, depth)], W[2, g, :, ds(col(i) * CT, CT)],
                                  preferred_element_type=F32)
        S[pl.ds(i, 1)] = part[:half][None]
        for r in range(1, inner):
            PS[i, r - 1] = part[r * half:(r + 1) * half].astype(BF)

        @pl.when(i > 0)
        def _():
            for r in range(1, inner):
                y_out(i - 1, r).start()
        return c
    lax.fori_loop(0, NT, produce, 0)
    for r in range(1, inner):
        y_out(NT - 1, r).start()
    for g in range(n_gr):
        out_tall(g).start()

    for q in range(1, n_tp):
        part = SH.at[(tp + n_tp - q) % n_tp]
        remote(part, part, sh_send.at[q - 1], sh_recv.at[q - 1], (gr, fs, (tp + q) % n_tp)).wait_recv()
    total = jnp.zeros((n_tp * R, cols), F32)
    su_n = GS.shape[1]
    for t in range(n_tp):
        total = total + jnp.dot(SH[t], DS[pl.ds(t * su_n, su_n), :], preferred_element_type=F32)
    SO[...] = total

    def z_move(way, i, lo, size, to):
        return remote(ZS.at[way, i, pl.ds(lo, size), :], ZR.at[way, i, pl.ds(lo, size), :],
                      z_send.at[way, i], z_recv.at[way, i], (gr, to * inner + y, tp))

    def upward(i, h):
        lo, size = (h + 1) * R, (nz - 1 - h) * R
        if h > 0:
            z_move(0, i, h * R, (nz - h) * R, z + 1).wait_recv()
            S[i, pl.ds(h * R, R), :] = S[i, pl.ds(h * R, R), :] + ZR[0, i, pl.ds(h * R, R), :].astype(F32)
            ZS[0, i, pl.ds(lo, size), :] = (
                S[i, pl.ds(lo, size), :] + ZR[0, i, pl.ds(lo, size), :].astype(F32)).astype(BF)
        else:
            ZS[0, i, pl.ds(lo, size), :] = S[i, pl.ds(lo, size), :].astype(BF)
        z_move(0, i, lo, size, z + 1).start()

    def downward(i, h):
        zz = nz - 1 - h
        size = zz * R
        if h > 0:
            z_move(1, i, 0, size + R, z - 1).wait_recv()
            S[i, pl.ds(size, R), :] = S[i, pl.ds(size, R), :] + ZR[1, i, pl.ds(size, R), :].astype(F32)
            ZS[1, i, pl.ds(0, size), :] = (
                S[i, pl.ds(0, size), :] + ZR[1, i, pl.ds(0, size), :].astype(F32)).astype(BF)
        else:
            ZS[1, i, pl.ds(0, size), :] = S[i, pl.ds(0, size), :].astype(BF)
        z_move(1, i, 0, size, z - 1).start()

    def f_copy(i, to):
        return remote(FS.at[i], FR.at[tp, i % tiles], f_send.at[i], f_recv.at[tp, i % tiles], (gr, fs, to))

    def finish(i):
        if nz > 1:
            last = (nz - 1) * R

            @pl.when(z == nz - 1)
            def _():
                z_move(0, i, last, R, z - 1).wait_recv()
                S[i, pl.ds(last, R), :] = S[i, pl.ds(last, R), :] + ZR[0, i, pl.ds(last, R), :].astype(F32)

            @pl.when(z == 0)
            def _():
                z_move(1, i, 0, R, z + 1).wait_recv()
                S[i, pl.ds(0, R), :] = S[i, pl.ds(0, R), :] + ZR[1, i, pl.ds(0, R), :].astype(F32)
        mine = S[i, ds(z * R, R), :]

        @pl.when(i < tiles)
        def _():
            at_cols = ds(i * CT, CT)
            mixed_o[tp, :, at_cols] = (mine + SO[ds(tp * R, R), at_cols]).astype(BF)

        @pl.when(i >= tiles)
        def _():
            FS[i] = mine.astype(BF)
            f_copy(i, col(i) // tiles).start()

    def advance(j, c):
        @pl.when(j < NT)
        def _():
            for r in range(1, inner):
                part = YR.at[j, r - 1]
                remote(part, part, y_send.at[j, r - 1], y_recv.at[j, r - 1],
                       (gr, z * inner + (y + r) % inner, tp)).wait_recv()
            S[j] = S[j] + sum([YR[j, r - 1].astype(F32) for r in range(1, inner)], 0.0)
        for h in range(nz - 1):
            i = j - h

            @pl.when((i >= 0) & (i < NT))
            def _(i=i, h=h):
                pl.when(z == h)(lambda: upward(i, h))
                pl.when(z == nz - 1 - h)(lambda: downward(i, h))
        i = j - (nz - 1)
        pl.when(i >= 0)(lambda: finish(i))
        return c
    lax.fori_loop(0, NT + nz - 1, advance, 0)

    def arrive(i, c):
        for q in range(1, n_tp):
            t = (tp + n_tp - q) % n_tp
            part = FR.at[t, i]
            remote(part, part, f_send.at[0], f_recv.at[t, i], (gr, fs, t)).wait_recv()
            at_cols = ds(i * CT, CT)
            mixed_o[t, :, at_cols] = (FR[t, i].astype(F32) + SO[ds(t * R, R), at_cols]).astype(BF)
        return c
    lax.fori_loop(0, tiles, arrive, 0)

    for m in range(3):
        part = locs[m].at[pl.ds(0, n_fs - 1)]
        remote(part, part, b_send.at[m], b_send.at[m], (gr, fs, (tp + 1) % n_tp)).wait_send()
        for q in range(1, n_tp):
            part = region(m, gr, tp)
            remote(part, part, x_send.at[m, q - 1], x_recv.at[m, q - 1],
                   (gr, fs, (tp + q) % n_tp)).wait_send()
        for q in range(n_tp):
            for p in range(1, n_gr):
                partner(m, gr, q, p).wait_send()
    for m in range(4):
        gather_sent(m)
        partner_gathered(m, 1)
    for q in range(1, n_tp):
        sh_copy(q).wait_send()

    def drain(i, c):
        for r in range(1, inner):
            y_out(i, r).wait_send()
        for h in range(nz - 1):
            pl.when(z == h)(lambda h=h: z_move(0, i, (h + 1) * R, (nz - 1 - h) * R, z + 1).wait_send())
            pl.when(z == nz - 1 - h)(lambda h=h: z_move(1, i, 0, (nz - 1 - h) * R, z - 1).wait_send())
        pl.when(i >= tiles)(lambda: f_copy(i, col(i) // tiles).wait_send())
        return c
    lax.fori_loop(0, NT, drain, 0)
    for g in range(n_gr):
        out_tall(g).wait()
        for m in (0, 1):
            out_wide(m, g).wait()
    for c in shared_outs:
        c.wait()


class Config:
    pass


def on_device(tokens, routes, route_weight, norm_gain, gate_experts, up_experts, down_experts,
              gate_shared, up_shared, down_shared):
    dims = (lax.axis_size("gr"), lax.axis_size("fs"), lax.axis_size("tp"))
    n_gr, n_fs, n_tp = dims
    fs_index = lax.axis_index("fs")
    tp_index = lax.axis_index("tp")
    per_group, rows, cols = gate_experts.shape[1:]
    count = per_group * n_gr
    assert per_group == n_fs
    tok_count, top = routes.shape
    width = tokens.shape[1]
    depth = rows * n_fs
    units = depth // n_tp

    cfg = Config()
    cfg.dims = dims
    cfg.inner = 2 if n_fs % 2 == 0 else 1
    cfg.nz = n_fs // cfg.inner
    part = tok_count // n_tp
    cfg.R = R = -(-part // 16) * 16
    cfg.CT = min(256, cols)
    cfg.NT = width // cfg.CT
    cfg.NB = min(256, depth)
    cfg.extra = extra = -(-2 * count // 128) * 128

    values = tokens.astype(F32)
    normed = (values * lax.rsqrt(jnp.mean(values * values, axis=-1, keepdims=True) + EPS)).astype(BF)
    named = routes[:, :, None] == jnp.arange(count, dtype=jnp.int32)[None, None, :]
    weight = jnp.sum(jnp.where(named, route_weight[:, :, None], 0.0), axis=1)
    high = lax.reduce_precision(weight, 8, 7)
    tail = jnp.concatenate(
        [high.astype(BF), (weight - high).astype(BF), jnp.zeros((tok_count, extra - 2 * count), BF)], axis=1)

    def in_parts(a):
        a = a.reshape(n_tp, part, a.shape[-1])
        return jnp.pad(a, ((0, 0), (0, R - part), (0, 0)))
    local = in_parts(normed)
    rows_here = lax.dynamic_index_in_dim(
        jnp.concatenate([local, in_parts(tail)], axis=2), tp_index, 0, keepdims=False)
    local = local.reshape(n_tp * R, width)

    gain_shared = lax.dynamic_slice_in_dim(
        norm_gain, fs_index * gate_shared.shape[0], gate_shared.shape[0], 0)
    gs = (gate_shared * gain_shared[:, None]).astype(BF)
    us = (up_shared * gain_shared[:, None]).astype(BF)
    dsh = down_shared.astype(BF)
    gain_cols = lax.dynamic_slice_in_dim(norm_gain, tp_index * cols, cols, 0)
    gate = (gate_experts[0] * gain_cols[None, None, :]).astype(BF)
    upper = (up_experts[0] * gain_cols[None, None, :]).astype(BF)
    down = down_experts[0].astype(BF)
    cfg.parts = tuple(n_gr if a.shape[0] % (16 * n_gr) == 0 else 1 for a in (gs, us, dsh))

    nz, inner, NT, CT = cfg.nz, cfg.inner, cfg.NT, cfg.CT
    tiles = NT // n_tp
    sds = jax.ShapeDtypeStruct
    outs = (
        sds((n_tp, R, cols), BF),
        sds((n_gr, 1, units, width), BF),
        sds((n_gr, 1, units, width), BF),
        sds((n_gr, 1, depth, cols), BF),
        sds((n_fs * gs.shape[0], gs.shape[1]), BF),
        sds((n_fs * us.shape[0], us.shape[1]), BF),
        sds((n_fs * dsh.shape[0], dsh.shape[1]), BF),
    )
    V, DMA = pltpu.VMEM, pltpu.SemaphoreType.DMA
    q, p, r = max(1, n_tp - 1), max(1, n_gr - 1), max(1, inner - 1)
    scratch = [
        V((n_fs * R, width + extra), BF),
        V((3, n_gr, depth, width), BF),
        V((n_fs * R, n_gr * depth), BF),
        V(outs[4].shape, BF), V(outs[5].shape, BF), V(outs[6].shape, BF),
        V((n_tp, n_tp * R, gs.shape[1]), BF),
        V((n_tp * R, cols), F32),
        V((NT, r, nz * R, CT), BF), V((NT, r, nz * R, CT), BF),
        V((NT, nz * R, CT), F32),
        V((2, NT, nz * R, CT), BF), V((2, NT, nz * R, CT), BF),
        V((NT, R, CT), BF), V((n_tp, tiles, R, CT), BF),
        DMA((3,)), DMA((3, n_fs)), DMA((3,)), DMA((3, q)), DMA((3, q)),
        DMA((3, n_tp, p)), DMA((3, n_tp, p)),
        DMA((4, 2, nz)), DMA((4, 2, nz)), DMA((4, r, 2 * nz - 1)), DMA((4, r, 2 * nz - 1)),
        DMA((4,)), DMA((4, p)), DMA((4, p)),
        DMA((q,)), DMA((q,)), DMA((NT, r)), DMA((NT, r)), DMA((2, NT)), DMA((2, NT)),
        DMA((NT,)), DMA((n_tp, tiles)), DMA((6, n_gr)),
    ]
    anyw = pl.BlockSpec(memory_space=pl.ANY)
    vmem = pl.BlockSpec(memory_space=pltpu.VMEM)
    mixed, gate_w, up_w, down_w, gs_w, us_w, ds_w = pl.pallas_call(
        functools.partial(whole, cfg),
        out_shape=outs,
        in_specs=[anyw, vmem] + [anyw] * 6,
        out_specs=(vmem,) + (anyw,) * 6,
        scratch_shapes=scratch,
        compiler_params=pltpu.CompilerParams(
            collective_id=1, has_side_effects=True, vmem_limit_bytes=60 << 20),
        cost_estimate=pl.CostEstimate(flops=0, bytes_accessed=200 << 20, transcendentals=0),
    )(rows_here, local, gate, upper, down, gs, us, dsh)
    mixed = mixed[:, :part].reshape(tok_count, cols)
    return (mixed, gate_w, up_w, down_w, gs_w, us_w, ds_w)


def solution(mesh):
    return jax.shard_map(
        on_device,
        mesh=mesh,
        in_specs=(
            P(("gr", "fs"), None),
            P(("gr", "fs"), None),
            P(("gr", "fs"), None),
            P(),
            P("gr", None, "fs", "tp"),
            P("gr", None, "fs", "tp"),
            P("gr", None, "fs", "tp"),
            P("fs", "tp"),
            P("fs", "tp"),
            P("fs", "tp"),
        ),
        out_specs=(
            P(("gr", "fs"), "tp"),
            P(None, "fs", "tp", None),
            P(None, "fs", "tp", None),
            P(None, "fs", None, "tp"),
            P(None, "tp"),
            P(None, "tp"),
            P(None, "tp"),
        ),
        check_vma=False,
    )
```

```python
import functools

import jax
import jax.numpy as jnp
from jax import lax
from jax.experimental import pallas as pl
from jax.experimental.pallas import tpu as pltpu
from jax.sharding import PartitionSpec as P

EPS = 1e-06
MESH = pl.DeviceIdType.MESH
BF = jnp.bfloat16
F32 = jnp.float32


def whole(cfg, tok_in, route_in, weight_in, gain_in, gate_in, up_in, down_in, gs_in, us_in, ds_in,
          mixed_o, gate_o, up_o, down_o, gs_o, us_o, ds_o,
          X, W, H, GS, US, DS, SH, SO, PS, YR, S, ZS, ZR, FS, FR, ST, LB, LG, LU, LD, LN,
          st_sem, b_send, b_recv, b_own, x_send, x_recv, p_send, p_recv,
          c_zs, c_zr, c_ys, c_yr, c_own, g_send, g_recv,
          sh_send, sh_recv, y_send, y_recv, z_send, z_recv, f_send, f_recv, o_sem):
    n_gr, n_fs, n_tp = cfg.dims
    inner, nz, R, NT, CT, DG = cfg.inner, cfg.nz, cfg.R, cfg.NT, cfg.CT, cfg.DG
    gr, fs, tp = lax.axis_index("gr"), lax.axis_index("fs"), lax.axis_index("tp")
    z, y = fs // inner, fs % inner
    rows, cols = gate_in.shape[1], gate_in.shape[2]
    width = cols * n_tp
    depth = rows * n_fs
    units = depth // n_tp
    count = n_gr * n_fs
    half = nz * R

    def ds(start, size):
        if isinstance(start, int):
            return pl.ds(start, size)
        return pl.ds(pl.multiple_of(start * 1, size), size)

    def remote(src, dst, s, r, to):
        return pltpu.make_async_remote_copy(
            src_ref=src, dst_ref=dst, send_sem=s, recv_sem=r, device_id=to, device_id_type=MESH)

    barrier = pltpu.get_barrier_semaphore()

    def greet(d, c):
        pl.semaphore_signal(barrier, inc=1, device_id=(gr, (fs + d) % n_fs, tp), device_id_type=MESH)
        return c
    lax.fori_loop(1, n_fs, greet, 0)
    for q in range(1, n_tp):
        pl.semaphore_signal(barrier, inc=1, device_id=(gr, fs, (tp + q) % n_tp), device_id_type=MESH)
    for p in range(1, n_gr):
        pl.semaphore_signal(barrier, inc=1, device_id=((gr + p) % n_gr, fs, tp), device_id_type=MESH)

    def stage(m):
        return pltpu.make_async_copy((gate_in, up_in, down_in)[m], ST.at[m % 2], st_sem.at[m])
    stage(0).start()
    stage(1).start()

    def normalize(i, c):
        at_rows = ds(i * 16, 16)
        v = tok_in[at_rows, :].astype(F32)
        v = v * lax.rsqrt(jnp.mean(v * v, axis=-1, keepdims=True) + EPS)
        LN[at_rows, :] = v.astype(BF)
        return c
    lax.fori_loop(0, n_tp * R // 16, normalize, 0)
    mine = ds(tp * R, R)
    X[ds(z * R, R), pl.ds(0, width)] = LN[mine, :]
    named, shares = route_in[mine, :], weight_in[mine, :]
    lane = lax.broadcasted_iota(jnp.int32, (R, cfg.extra), 1)
    tail = jnp.zeros((R, cfg.extra), F32)
    for j in range(named.shape[1]):
        e, w = named[:, j:j + 1], shares[:, j:j + 1]
        high = w.astype(BF).astype(F32)
        tail = tail + jnp.where(lane == e, high, 0.0) + jnp.where(lane == e + count, w - high, 0.0)
    X[ds(z * R, R), pl.ds(width, cfg.extra)] = tail.astype(BF)

    gain = gain_in[:, ds(tp * cols, cols)]

    def convert(m):
        stage(m).wait()

        def one(k, c):
            v = ST[m % 2, k]
            LB[m, k] = (v * gain if m < 2 else v).astype(BF)
            return c
        lax.fori_loop(0, n_fs, one, 0)
    convert(0)
    stage(2).start()

    gw = cols // DG

    def span(m):
        return (0, cols) if m < 2 else ((m - 2) * gw, gw)

    def block(m, s, t):
        lo, size = span(m)
        return W.at[min(m, 2), gr, ds(s * rows, rows), pl.ds(pl.multiple_of(t * cols + lo, size), size)]

    def region(m, g, t):
        lo, size = span(m)
        return W.at[min(m, 2), g, :, pl.ds(pl.multiple_of(t * cols + lo, size), size)]

    def local(m, k):
        lo, size = span(m)
        return LB.at[min(m, 2), k, :, pl.ds(lo, size)]

    def to_expert(m, k):
        return remote(local(m, k), block(m, fs, tp), b_send.at[m], b_recv.at[m, fs], (gr, k, tp))

    def own_block(m):
        return pltpu.make_async_copy(local(m, fs), block(m, fs, tp), b_own.at[m])

    def each_other(act, lo=1, hi=n_fs):
        def step(d, c):
            pl.when(fs + d < n_fs)(lambda: act(fs + d))
            pl.when(fs - d >= 0)(lambda: act(fs - d))
            return c
        lax.fori_loop(lo, hi, step, 0)

    def across(m, src, s):
        for q in range(1, n_tp):
            remote(src, block(m, s, tp), x_send.at[m, q - 1], x_recv.at[m, q - 1],
                   (gr, fs, (tp + q) % n_tp)).start()

    def keep_own(m):
        own_block(m).start()
        across(m, local(m, fs), fs)

    def send(m, k):
        to_expert(m, k).start()

    def landed(m, s):
        part = block(m, s, tp)
        remote(part, part, b_recv.at[m, s], b_recv.at[m, s], (gr, s, tp)).wait_recv()
        across(m, part, s)

    def partner(m, g, q, p):
        part = region(m, g, (tp + n_tp - q) % n_tp)
        return remote(part, part, p_send.at[m, q, p - 1], p_recv.at[m, q, p - 1],
                      ((gr + p) % n_gr, fs, tp))

    def share(m, q):
        for p in range(1, n_gr):
            partner(m, gr, q, p).start()

    def shared_landed(m, q):
        for p in range(1, n_gr):
            partner(m, (gr + n_gr - p) % n_gr, q, p).wait_recv()

    def x_landed(m, q):
        part = region(m, gr, (tp + n_tp - q) % n_tp)
        remote(part, part, x_send.at[m, q - 1], x_recv.at[m, q - 1],
               (gr, fs, (tp + q) % n_tp)).wait_recv()

    def token_place(zz, yr):
        return X.at[ds((yr * nz + zz) * R, R), :]

    def shared_item(src, dst, parts):
        size = src.shape[0] // parts

        def place(zz, yr):
            f = zz * inner + (y + yr) % inner
            if parts == 1:
                return dst.at[ds(f * size, size), :]
            return dst.at[ds((f * parts + gr) * size, size), :]
        return (src if parts == 1 else src.at[ds(gr * size, size), :], place, parts)
    items = ((token_place(z, 0), token_place, 1),) + tuple(
        shared_item(s, d, p) for s, d, p in zip((LG, LU, LD), (GS, US, DS), cfg.parts))

    def at(way, d):
        return z - d if way == 0 else z + d

    def z_copy(m, way, d):
        own, place, _ = items[m]
        dst = place(at(way, d), 0)
        return remote(own if d == 0 else dst, dst, c_zs.at[m, way, d], c_zr.at[m, way, d],
                      (gr, (z + 1 if way == 0 else z - 1) * inner + y, tp))

    def y_slot(d, way):
        return d + way * (nz - 1) if d else 0

    def y_copy(m, q, way, d):
        own, place, parts = items[m]
        zz = at(way, d)
        src = own if d == 0 else place(zz, 0)
        dst = place(zz, inner - q) if m == 0 else place(zz, 0)
        i = y_slot(d, way)
        return remote(src, dst, c_ys.at[m, q - 1, i], c_yr.at[m, q - 1, i],
                      (gr, z * inner + (y + q) % inner, tp))

    def pass_partner(m, part):
        if items[m][2] > 1:
            for p in range(1, n_gr):
                remote(part, part, g_send.at[m, p - 1], g_recv.at[m, p - 1],
                       ((gr + p) % n_gr, fs, tp)).start()

    def next_there(way):
        return (z < nz - 1) if way == 0 else (z > 0)

    def there(d, way):
        return (z - d >= 0) if way == 0 else (z + d < nz)

    def gather_start(m):
        own, place, parts = items[m]
        for way in (0, 1):
            pl.when(next_there(way))(lambda way=way: z_copy(m, way, 0).start())
        for q in range(1, inner):
            y_copy(m, q, 0, 0).start()
        if m:
            pltpu.make_async_copy(own, place(z, 0), c_own.at[m]).start()

    def gather_own(m):
        own, place, parts = items[m]
        pltpu.make_async_copy(own, place(z, 0), c_own.at[m]).wait()
        pass_partner(m, place(z, 0))

    def gather_pass(m, d):
        for way in (0, 1):
            def act(way=way):
                part = items[m][1](at(way, d), 0)
                remote(part, part, c_zs.at[m, way, d - 1], c_zr.at[m, way, d - 1],
                       (gr, (z + 1 if way == 0 else z - 1) * inner + y, tp)).wait_recv()
                if d < nz - 1:
                    pl.when(next_there(way))(lambda: z_copy(m, way, d).start())
                for q in range(1, inner):
                    y_copy(m, q, way, d).start()
                pass_partner(m, part)
            pl.when(there(d, way))(act)

    places = [(0, 0)] + [(d, way) for d in range(1, nz) for way in (0, 1)]

    def gather_y(m):
        for d, way in places:
            def act(d=d, way=way):
                for q in range(1, inner):
                    part = items[m][1](at(way, d), inner - q)
                    i = y_slot(d, way)
                    remote(part, part, c_ys.at[m, q - 1, i], c_yr.at[m, q - 1, i],
                           (gr, z * inner + (y + q) % inner, tp)).wait_recv()
                    pass_partner(m, part)
            if d == 0:
                act()
            else:
                pl.when(there(d, way))(act)

    def gather_sent(m):
        for d, way in places:
            def act(d=d, way=way):
                for w in ((0, 1) if d == 0 else (way,)):
                    if d < nz - 1:
                        pl.when(next_there(w))(lambda w=w: z_copy(m, w, d).wait_send())
                for q in range(1, inner):
                    y_copy(m, q, way, d).wait_send()
            if d == 0:
                act()
            else:
                pl.when(there(d, way))(act)

    def partner_gathered(m, way):
        dst = (X, GS, US, DS)[m]
        if items[m][2] > 1:
            part = dst.at[pl.ds(0, dst.shape[0] // items[m][2]), :]
            for p in range(1, n_gr):
                c = remote(part, part, g_send.at[m, p - 1], g_recv.at[m, p - 1],
                           ((gr + p) % n_gr, fs, tp))
                if way:
                    c.wait_send()
                else:
                    c.wait_recv()

    per = depth // CT
    chunks = n_gr * per
    lanes = lax.broadcasted_iota(jnp.int32, (n_fs * R, cfg.extra), 1)
    dn = (((1,), (1,)), ((), ()))

    def gate_product(i, c):
        gg, n = (gr + i // per) % n_gr, i % per
        v = lax.dot_general(X[:, pl.ds(0, width)], W[0, gg, ds(n * CT, CT), :], dn,
                            preferred_element_type=F32)
        for r in range(inner):
            S[i * inner + r] = v[r * half:(r + 1) * half]
        return c

    def up_product(i, c):
        gg, n = (gr + i // per) % n_gr, i % per
        v = lax.dot_general(X[:, pl.ds(0, width)], W[1, gg, ds(n * CT, CT), :], dn,
                            preferred_element_type=F32)
        expert = gg * n_fs + fs
        pick = (lanes == expert) | (lanes == count + expert)
        weight = jnp.sum(jnp.where(pick, X[:, pl.ds(width, cfg.extra)].astype(F32), 0.0),
                         axis=1, keepdims=True)
        for r in range(inner):
            part = slice(r * half, (r + 1) * half)
            gate = S[i * inner + r]
            H[pl.ds(r * half, half), ds((gg * per + n) * CT, CT)] = (
                gate / (1.0 + jnp.exp(-gate)) * v[part] * weight[part]).astype(BF)
        return c

    pl.semaphore_wait(barrier, n_fs - 1 + n_tp - 1 + n_gr - 1)
    stops = max(1, nz - 1)
    size = -(-(n_fs - 1) // stops)
    parts = [(1 + k * size, min(n_fs, 1 + (k + 1) * size)) for k in range(stops)]
    gather_start(0)
    keep_own(0)
    each_other(lambda k: send(0, k), *parts[0])
    convert(1)
    keep_own(1)
    at_row = lax.broadcasted_iota(jnp.int32, (LG.shape[0], width), 0) + fs * LG.shape[0]
    at_col = lax.broadcasted_iota(jnp.int32, (LG.shape[0], width), 1)
    gain_rows = jnp.sum(jnp.where(at_row == at_col, gain_in[...], 0.0), axis=1, keepdims=True)
    LG[...] = (gs_in[...] * gain_rows).astype(BF)
    LU[...] = (us_in[...] * gain_rows).astype(BF)
    LD[...] = ds_in[...].astype(BF)
    convert(2)
    if nz > 1:
        gather_pass(0, 1)
    for part in parts[1:]:
        each_other(lambda k: send(0, k), *part)

    def second(s):
        landed(1, s)
        send(2, s)
    for k, part in enumerate(parts):
        each_other(lambda s: landed(0, s), *part)
        if k + 2 < nz - 1 or k + 2 == nz - 1 == 2:
            gather_pass(0, k + 2)
        each_other(lambda s: send(1, s), *part)
    own_block(0).wait()
    share(0, 0)
    for m in range(2, 2 + DG):
        keep_own(m)
    for m in (1, 2, 3):
        gather_start(m)
    for k, part in enumerate(parts):
        each_other(second, *part)
        if k == 0:
            if nz > 3:
                gather_pass(0, nz - 1)
            for m in (1, 2, 3):
                gather_own(m)
            for q in range(1, n_tp):
                x_landed(0, q)
                share(0, q)
        if k == max(0, stops - 2):
            gather_y(0)
            lax.fori_loop(0, per, gate_product, 0)
    shared_pass = [(lambda d=d: [gather_pass(m, d) for m in (1, 2, 3)]) for d in range(1, nz)]
    for d in range(0, max(0, nz - 3)):
        shared_pass[d]()
    for m in range(3, 2 + DG):
        each_other(lambda k: send(m, k))
    own_block(1).wait()
    share(1, 0)
    for q in range(n_tp):
        shared_landed(0, q)
    lax.fori_loop(per, chunks, gate_product, 0)
    for q in range(1, n_tp):
        x_landed(1, q)
        share(1, q)
    for d in range(max(0, nz - 3), max(0, nz - 2)):
        shared_pass[d]()

    def out_wide(m, g):
        return pltpu.make_async_copy(
            W.at[m, g, ds(tp * units, units), :], (gate_o, up_o)[m].at[g, 0], o_sem.at[m, g])

    def out_tall(g):
        return pltpu.make_async_copy(
            W.at[2, g, :, ds(tp * cols, cols)], down_o.at[g, 0], o_sem.at[2, g])

    for g in range(n_gr):
        out_wide(0, g).start()

    each = -(-(n_fs - 1) // chunks)

    def ahead(i, c):
        up_product(i, 0)
        each_other(lambda s: landed(2, s), 1 + i * each, jnp.minimum(n_fs, 1 + (i + 1) * each))
        return c
    lax.fori_loop(0, per, ahead, 0)
    for q in range(n_tp):
        shared_landed(1, q)
    for g in range(n_gr):
        out_wide(1, g).start()
    for d in range(max(0, nz - 2), nz - 1):
        shared_pass[d]()
    lax.fori_loop(per, chunks, ahead, 0)

    tiles = NT // n_tp
    each_group = tiles // DG
    group = n_tp * each_group

    def owner(i):
        return (tp + i // each_group % n_tp) % n_tp

    def place_in(i):
        return i // group * each_group + i % each_group

    def y_out(i, r):
        return remote(PS.at[i, r - 1], YR.at[i, r - 1], y_send.at[i, r - 1], y_recv.at[i, r - 1],
                      (gr, z * inner + (y + r) % inner, tp))

    def produce(i, c):
        at_cols = ds((owner(i) * tiles + place_in(i)) * CT, CT)
        part = jnp.zeros((n_fs * R, CT), F32)
        for g in range(n_gr):
            part = part + jnp.dot(H[:, pl.ds(g * depth, depth)], W[2, g, :, at_cols],
                                  preferred_element_type=F32)
        S[i] = part[:half]
        for r in range(1, inner):
            PS[i, r - 1] = part[r * half:(r + 1) * half].astype(BF)

        @pl.when(i % each_group > 0)
        def _():
            for r in range(1, inner):
                y_out(i - 1, r).start()
        return c

    def tell(i):
        for r in range(1, inner):
            y_out(i, r).start()

    def make(a, u):
        m = 2 + a
        if u:
            x_landed(m, u)
        else:
            own_block(m).wait()
        share(m, u)
        shared_landed(m, u)
        base = (a * n_tp + (n_tp - u) % n_tp) * each_group
        lax.fori_loop(base, base + each_group, produce, 0)
        tell(base + each_group - 1)

    turn = [0] + [n_tp - u for u in range(1, n_tp)]
    for u in turn:
        make(0, u)

    for m in (1, 2, 3):
        gather_y(m)
        partner_gathered(m, 0)
    sg = jnp.dot(LN[...], GS[...], preferred_element_type=F32)
    su = jnp.dot(LN[...], US[...], preferred_element_type=F32)
    SH[tp] = (sg / (1.0 + jnp.exp(-sg)) * su).astype(BF)
    shared_outs = [pltpu.make_async_copy(a, b, o_sem.at[3 + i, 0])
                   for i, (a, b) in enumerate(((GS, gs_o), (US, us_o), (DS, ds_o)))]
    for c in shared_outs:
        c.start()

    def sh_copy(q):
        return remote(SH.at[tp], SH.at[tp], sh_send.at[q - 1], sh_recv.at[q - 1],
                      (gr, fs, (tp + q) % n_tp))
    for q in range(1, n_tp):
        sh_copy(q).start()

    def shared_rest():
        for q in range(1, n_tp):
            part = SH.at[(tp + n_tp - q) % n_tp]
            remote(part, part, sh_send.at[q - 1], sh_recv.at[q - 1], (gr, fs, (tp + q) % n_tp)).wait_recv()
        total = jnp.zeros((n_tp * R, cols), F32)
        su_n = GS.shape[1]
        for t in range(n_tp):
            total = total + jnp.dot(SH[t], DS[pl.ds(t * su_n, su_n), :], preferred_element_type=F32)
        SO[...] = total

    def z_move(way, i, lo, size, to):
        return remote(ZS.at[way, i, pl.ds(lo, size), :], ZR.at[way, i, pl.ds(lo, size), :],
                      z_send.at[way, i], z_recv.at[way, i], (gr, to * inner + y, tp))

    def upward(i, h):
        lo, size = (h + 1) * R, (nz - 1 - h) * R
        if h > 0:
            z_move(0, i, h * R, (nz - h) * R, z + 1).wait_recv()
            S[i, pl.ds(h * R, R), :] = S[i, pl.ds(h * R, R), :] + ZR[0, i, pl.ds(h * R, R), :].astype(F32)
            ZS[0, i, pl.ds(lo, size), :] = (
                S[i, pl.ds(lo, size), :] + ZR[0, i, pl.ds(lo, size), :].astype(F32)).astype(BF)
        else:
            ZS[0, i, pl.ds(lo, size), :] = S[i, pl.ds(lo, size), :].astype(BF)
        z_move(0, i, lo, size, z + 1).start()

    def downward(i, h):
        zz = nz - 1 - h
        size = zz * R
        if h > 0:
            z_move(1, i, 0, size + R, z - 1).wait_recv()
            S[i, pl.ds(size, R), :] = S[i, pl.ds(size, R), :] + ZR[1, i, pl.ds(size, R), :].astype(F32)
            ZS[1, i, pl.ds(0, size), :] = (
                S[i, pl.ds(0, size), :] + ZR[1, i, pl.ds(0, size), :].astype(F32)).astype(BF)
        else:
            ZS[1, i, pl.ds(0, size), :] = S[i, pl.ds(0, size), :].astype(BF)
        z_move(1, i, 0, size, z - 1).start()

    def f_copy(i):
        return remote(FS.at[i], FR.at[tp, place_in(i)], f_send.at[i], f_recv.at[tp, place_in(i)],
                      (gr, fs, owner(i)))

    def is_mine(i):
        return i // each_group % n_tp == 0

    def finish(i):
        if nz > 1:
            last = (nz - 1) * R

            @pl.when(z == nz - 1)
            def _():
                z_move(0, i, last, R, z - 1).wait_recv()
                S[i, pl.ds(last, R), :] = S[i, pl.ds(last, R), :] + ZR[0, i, pl.ds(last, R), :].astype(F32)

            @pl.when(z == 0)
            def _():
                z_move(1, i, 0, R, z + 1).wait_recv()
                S[i, pl.ds(0, R), :] = S[i, pl.ds(0, R), :] + ZR[1, i, pl.ds(0, R), :].astype(F32)
        done = S[i, ds(z * R, R), :]

        @pl.when(is_mine(i))
        def _():
            at_cols = ds(place_in(i) * CT, CT)
            mixed_o[tp, :, at_cols] = (done + SO[ds(tp * R, R), at_cols]).astype(BF)

        @pl.when(jnp.logical_not(is_mine(i)))
        def _():
            FS[i] = done.astype(BF)
            f_copy(i).start()

    turns = 3 if DG > 1 else 0
    some = -(-(n_fs - 1) // 3)

    def advance(j, c):
        if DG > 1:
            @pl.when(j < turns)
            def _():
                each_other(lambda s: landed(3, s), jnp.minimum(n_fs, 1 + j * some),
                           jnp.minimum(n_fs, 1 + (j + 1) * some))
            for k, u in enumerate(turn):
                pl.when(j == turns + k)(lambda u=u: make(1, u))
        pl.when(j == min(2, max(0, nz - 2)))(shared_rest)

        @pl.when(j < NT)
        def _():
            for r in range(1, inner):
                part = YR.at[j, r - 1]
                remote(part, part, y_send.at[j, r - 1], y_recv.at[j, r - 1],
                       (gr, z * inner + (y + r) % inner, tp)).wait_recv()
            S[j] = S[j] + sum([YR[j, r - 1].astype(F32) for r in range(1, inner)], 0.0)
        for h in range(nz - 1):
            i = j - h

            @pl.when((i >= 0) & (i < NT))
            def _(i=i, h=h):
                pl.when(z == h)(lambda: upward(i, h))
                pl.when(z == nz - 1 - h)(lambda: downward(i, h))
        i = j - (nz - 1)
        pl.when(i >= 0)(lambda: finish(i))
        return c
    lax.fori_loop(0, NT + nz - 1, advance, 0)
    for g in range(n_gr):
        out_tall(g).start()

    def arrive(i, c):
        for q in range(1, n_tp):
            t = (tp + n_tp - q) % n_tp
            part = FR.at[t, i]
            remote(part, part, f_send.at[0], f_recv.at[t, i], (gr, fs, t)).wait_recv()
            at_cols = ds(i * CT, CT)
            mixed_o[t, :, at_cols] = (FR[t, i].astype(F32) + SO[ds(t * R, R), at_cols]).astype(BF)
        return c
    lax.fori_loop(0, tiles, arrive, 0)

    for m in range(2 + DG):
        lo, size_m = span(m)
        part = LB.at[min(m, 2), pl.ds(0, n_fs - 1), :, pl.ds(lo, size_m)]
        remote(part, part, b_send.at[m], b_send.at[m], (gr, fs, (tp + 1) % n_tp)).wait_send()
        for q in range(1, n_tp):
            part = region(m, gr, tp)
            remote(part, part, x_send.at[m, q - 1], x_recv.at[m, q - 1],
                   (gr, fs, (tp + q) % n_tp)).wait_send()
        for q in range(n_tp):
            for p in range(1, n_gr):
                partner(m, gr, q, p).wait_send()
    for m in range(4):
        gather_sent(m)
        partner_gathered(m, 1)
    for q in range(1, n_tp):
        sh_copy(q).wait_send()

    def drain(i, c):
        for r in range(1, inner):
            y_out(i, r).wait_send()
        for h in range(nz - 1):
            pl.when(z == h)(lambda h=h: z_move(0, i, (h + 1) * R, (nz - 1 - h) * R, z + 1).wait_send())
            pl.when(z == nz - 1 - h)(lambda h=h: z_move(1, i, 0, (nz - 1 - h) * R, z - 1).wait_send())
        pl.when(jnp.logical_not(is_mine(i)))(lambda: f_copy(i).wait_send())
        return c
    lax.fori_loop(0, NT, drain, 0)
    for g in range(n_gr):
        out_tall(g).wait()
        for m in (0, 1):
            out_wide(m, g).wait()
    for c in shared_outs:
        c.wait()


class Config:
    pass


def on_device(tokens, routes, route_weight, norm_gain, gate_experts, up_experts, down_experts,
              gate_shared, up_shared, down_shared):
    dims = (lax.axis_size("gr"), lax.axis_size("fs"), lax.axis_size("tp"))
    n_gr, n_fs, n_tp = dims
    per_group, rows, cols = gate_experts.shape[1:]
    count = per_group * n_gr
    assert per_group == n_fs
    tok_count, top = routes.shape
    width = tokens.shape[1]
    depth = rows * n_fs
    units = depth // n_tp

    cfg = Config()
    cfg.dims = dims
    cfg.inner = inner = 2 if n_fs % 2 == 0 else 1
    cfg.nz = nz = n_fs // inner
    part = tok_count // n_tp
    cfg.R = R = -(-part // 16) * 16
    cfg.CT = CT = min(256, cols, depth)
    cfg.NT = NT = width // CT
    tiles = NT // n_tp
    cfg.DG = DG = 2 if tiles % 2 == 0 and tiles > 1 else 1
    cfg.extra = extra = -(-2 * count // 128) * 128
    chunks = n_gr * depth // CT

    def in_parts(a):
        if R == part:
            return a
        a = jnp.pad(a.reshape(n_tp, part, a.shape[-1]), ((0, 0), (0, R - part), (0, 0)))
        return a.reshape(n_tp * R, a.shape[-1])

    gs, us, dsh = gate_shared, up_shared, down_shared
    cfg.parts = tuple(n_gr if a.shape[0] % (16 * n_gr) == 0 else 1 for a in (gs, us, dsh))
    sds = jax.ShapeDtypeStruct
    outs = (
        sds((n_tp, R, cols), BF),
        sds((n_gr, 1, units, width), BF),
        sds((n_gr, 1, units, width), BF),
        sds((n_gr, 1, depth, cols), BF),
        sds((n_fs * gs.shape[0], gs.shape[1]), BF),
        sds((n_fs * us.shape[0], us.shape[1]), BF),
        sds((n_fs * dsh.shape[0], dsh.shape[1]), BF),
    )
    V, DMA = pltpu.VMEM, pltpu.SemaphoreType.DMA
    q, p, r = max(1, n_tp - 1), max(1, n_gr - 1), max(1, inner - 1)
    M = 2 + DG
    scratch = [
        V((n_fs * R, width + extra), BF),
        V((3, n_gr, depth, width), BF),
        V((n_fs * R, n_gr * depth), BF),
        V(outs[4].shape, BF), V(outs[5].shape, BF), V(outs[6].shape, BF),
        V((n_tp, n_tp * R, gs.shape[1]), BF),
        V((n_tp * R, cols), F32),
        V((NT, r, nz * R, CT), BF), V((NT, r, nz * R, CT), BF),
        V((max(NT, chunks * inner), nz * R, CT), F32),
        V((2, NT, nz * R, CT), BF), V((2, NT, nz * R, CT), BF),
        V((NT, R, CT), BF), V((n_tp, tiles, R, CT), BF),
        V((2, n_fs, rows, cols), F32), V((3, n_fs, rows, cols), BF),
        V(gs.shape, BF), V(us.shape, BF), V(dsh.shape, BF),
        V((n_tp * R, width), BF),
        DMA((3,)),
        DMA((M,)), DMA((M, n_fs)), DMA((M,)), DMA((M, q)), DMA((M, q)),
        DMA((M, n_tp, p)), DMA((M, n_tp, p)),
        DMA((4, 2, nz)), DMA((4, 2, nz)), DMA((4, r, 2 * nz - 1)), DMA((4, r, 2 * nz - 1)),
        DMA((4,)), DMA((4, p)), DMA((4, p)),
        DMA((q,)), DMA((q,)), DMA((NT, r)), DMA((NT, r)), DMA((2, NT)), DMA((2, NT)),
        DMA((NT,)), DMA((n_tp, tiles)), DMA((6, n_gr)),
    ]
    anyw = pl.BlockSpec(memory_space=pl.ANY)
    vmem = pl.BlockSpec(memory_space=pltpu.VMEM)
    held = pl.pallas_call(
        functools.partial(whole, cfg),
        out_shape=tuple(V(o.shape, o.dtype) for o in outs),
        in_specs=[vmem] * 4 + [anyw] * 3 + [vmem] * 3,
        out_specs=(vmem,) * 7,
        scratch_shapes=scratch,
        compiler_params=pltpu.CompilerParams(
            collective_id=1, has_side_effects=True, vmem_limit_bytes=48 << 20),
        cost_estimate=pl.CostEstimate(flops=0, bytes_accessed=200 << 20, transcendentals=0),
    )(in_parts(tokens), in_parts(routes), in_parts(route_weight), norm_gain.reshape(1, width),
      gate_experts[0], up_experts[0], down_experts[0], gs, us, dsh)
    mixed, gate_w, up_w, down_w, gs_w, us_w, ds_w = pl.pallas_call(
        put,
        out_shape=outs,
        in_specs=[vmem] * 7,
        out_specs=(anyw,) * 7,
        scratch_shapes=[DMA((7,))],
        compiler_params=pltpu.CompilerParams(vmem_limit_bytes=1 << 20),
        cost_estimate=pl.CostEstimate(flops=0, bytes_accessed=20 << 20, transcendentals=0),
    )(*held)
    mixed = mixed[:, :part].reshape(tok_count, cols)
    return (mixed, gate_w, up_w, down_w, gs_w, us_w, ds_w)


def put(*refs):
    sems = refs[-1]
    copies = [pltpu.make_async_copy(a, b, sems.at[i]) for i, (a, b) in enumerate(zip(refs[:7], refs[7:14]))]
    for c in copies:
        c.start()
    for c in copies:
        c.wait()


def solution(mesh):
    return jax.shard_map(
        on_device,
        mesh=mesh,
        in_specs=(
            P(("gr", "fs"), None),
            P(("gr", "fs"), None),
            P(("gr", "fs"), None),
            P(),
            P("gr", None, "fs", "tp"),
            P("gr", None, "fs", "tp"),
            P("gr", None, "fs", "tp"),
            P("fs", "tp"),
            P("fs", "tp"),
            P("fs", "tp"),
        ),
        out_specs=(
            P(("gr", "fs"), "tp"),
            P(None, "fs", "tp", None),
            P(None, "fs", "tp", None),
            P(None, "fs", None, "tp"),
            P(None, "tp"),
            P(None, "tp"),
            P(None, "tp"),
        ),
        check_vma=False,
    )
```

```python
import functools

import jax
import jax.numpy as jnp
from jax import lax
from jax.experimental import pallas as pl
from jax.experimental.pallas import tpu as pltpu
from jax.sharding import PartitionSpec as P

EPS = 1e-06
MESH = pl.DeviceIdType.MESH
BF = jnp.bfloat16
F32 = jnp.float32


def whole(cfg, tok_in, route_in, weight_in, gain_in, gate_in, up_in, down_in, gs_in, us_in, ds_in,
          mixed_o, gate_o, up_o, down_o, gs_o, us_o, ds_o,
          X, W, H, GS, US, DS, SH, SO, PS, YR, S, ZS, ZR, ZD, FS, FR, RO, ST, LB, LG, LU, LD, LN,
          st_sem, b_send, b_recv, b_own, x_send, x_recv, p_send, p_recv,
          c_zs, c_zr, c_ys, c_yr, c_own, g_send, g_recv,
          sh_send, sh_recv, y_send, y_recv, z_send, z_recv, d_send, d_recv, f_send, f_recv, o_sem):
    n_gr, n_fs, n_tp = cfg.dims
    inner, nz, R, NT, CT, DG = cfg.inner, cfg.nz, cfg.R, cfg.NT, cfg.CT, cfg.DG
    gr, fs, tp = lax.axis_index("gr"), lax.axis_index("fs"), lax.axis_index("tp")
    z, y = fs // inner, fs % inner
    rows, cols = gate_in.shape[1], gate_in.shape[2]
    width = cols * n_tp
    depth = rows * n_fs
    units = depth // n_tp
    count = n_gr * n_fs
    half = nz * R

    def ds(start, size):
        if isinstance(start, int):
            return pl.ds(start, size)
        return pl.ds(pl.multiple_of(start * 1, size), size)

    def remote(src, dst, s, r, to):
        return pltpu.make_async_remote_copy(
            src_ref=src, dst_ref=dst, send_sem=s, recv_sem=r, device_id=to, device_id_type=MESH)

    barrier = pltpu.get_barrier_semaphore()

    def greet(d, c):
        pl.semaphore_signal(barrier, inc=1, device_id=(gr, (fs + d) % n_fs, tp), device_id_type=MESH)
        return c
    lax.fori_loop(1, n_fs, greet, 0)
    for q in range(1, n_tp):
        pl.semaphore_signal(barrier, inc=1, device_id=(gr, fs, (tp + q) % n_tp), device_id_type=MESH)
    for p in range(1, n_gr):
        pl.semaphore_signal(barrier, inc=1, device_id=((gr + p) % n_gr, fs, tp), device_id_type=MESH)

    def stage(m):
        return pltpu.make_async_copy((gate_in, up_in, down_in)[m], ST.at[m % 2], st_sem.at[m])
    stage(0).start()
    stage(1).start()

    def normalize(i, c):
        at_rows = ds(i * 16, 16)
        v = tok_in[at_rows, :].astype(F32)
        v = v * lax.rsqrt(jnp.mean(v * v, axis=-1, keepdims=True) + EPS)
        LN[at_rows, :] = v.astype(BF)
        return c
    lax.fori_loop(0, n_tp * R // 16, normalize, 0)
    mine = ds(tp * R, R)
    X[ds(z * R, R), pl.ds(0, width)] = LN[mine, :]
    named, shares = route_in[mine, :], weight_in[mine, :]
    lane = lax.broadcasted_iota(jnp.int32, (R, cfg.extra), 1)
    tail = jnp.zeros((R, cfg.extra), F32)
    for j in range(named.shape[1]):
        e, w = named[:, j:j + 1], shares[:, j:j + 1]
        high = w.astype(BF).astype(F32)
        tail = tail + jnp.where(lane == e, high, 0.0) + jnp.where(lane == e + count, w - high, 0.0)
    X[ds(z * R, R), pl.ds(width, cfg.extra)] = tail.astype(BF)

    gain = gain_in[:, ds(tp * cols, cols)]

    def convert(m):
        stage(m).wait()

        def one(k, c):
            v = ST[m % 2, k]
            LB[m, k] = (v * gain if m < 2 else v).astype(BF)
            return c
        lax.fori_loop(0, n_fs, one, 0)
    convert(0)
    stage(2).start()

    gw = cols // DG

    def span(m):
        return (0, cols) if m < 2 else ((m - 2) * gw, gw)

    def block(m, s, t):
        lo, size = span(m)
        return W.at[min(m, 2), gr, ds(s * rows, rows), pl.ds(pl.multiple_of(t * cols + lo, size), size)]

    def region(m, g, t):
        lo, size = span(m)
        return W.at[min(m, 2), g, :, pl.ds(pl.multiple_of(t * cols + lo, size), size)]

    def local(m, k):
        lo, size = span(m)
        return LB.at[min(m, 2), k, :, pl.ds(lo, size)]

    def to_expert(m, k):
        return remote(local(m, k), block(m, fs, tp), b_send.at[m], b_recv.at[m, fs], (gr, k, tp))

    def own_block(m):
        return pltpu.make_async_copy(local(m, fs), block(m, fs, tp), b_own.at[m])

    def each_other(act, lo=1, hi=n_fs):
        def step(d, c):
            pl.when(fs + d < n_fs)(lambda: act(fs + d))
            pl.when(fs - d >= 0)(lambda: act(fs - d))
            return c
        lax.fori_loop(lo, hi, step, 0)

    def across(m, src, s):
        for q in range(1, n_tp):
            remote(src, block(m, s, tp), x_send.at[m, q - 1], x_recv.at[m, q - 1],
                   (gr, fs, (tp + q) % n_tp)).start()

    def keep_own(m):
        own_block(m).start()
        across(m, local(m, fs), fs)

    def send(m, k):
        to_expert(m, k).start()

    def landed(m, s):
        part = block(m, s, tp)
        remote(part, part, b_recv.at[m, s], b_recv.at[m, s], (gr, s, tp)).wait_recv()
        across(m, part, s)

    def partner(m, g, q, p):
        part = region(m, g, (tp + n_tp - q) % n_tp)
        return remote(part, part, p_send.at[m, q, p - 1], p_recv.at[m, q, p - 1],
                      ((gr + p) % n_gr, fs, tp))

    def share(m, q):
        for p in range(1, n_gr):
            partner(m, gr, q, p).start()

    def shared_landed(m, q):
        for p in range(1, n_gr):
            partner(m, (gr + n_gr - p) % n_gr, q, p).wait_recv()

    def x_landed(m, q):
        part = region(m, gr, (tp + n_tp - q) % n_tp)
        remote(part, part, x_send.at[m, q - 1], x_recv.at[m, q - 1],
               (gr, fs, (tp + q) % n_tp)).wait_recv()

    def token_place(zz, yr):
        return X.at[ds((yr * nz + zz) * R, R), :]

    def shared_item(src, dst):
        size = src.shape[0]

        def place(zz, yr):
            return dst.at[ds((zz * inner + (y + yr) % inner) * size, size), :]
        return (src, place)
    items = ((token_place(z, 0), token_place),) + tuple(
        shared_item(s, d) for s, d in zip((LG, LU, LD), (GS, US, DS)))
    carrier = gr == n_gr - 1

    def carried(f):
        def run(m, *rest):
            if m:
                pl.when(carrier)(lambda: f(m, *rest))
            else:
                f(m, *rest)
        return run

    def at(way, d):
        return z - d if way == 0 else z + d

    def z_copy(m, way, d):
        own, place = items[m]
        dst = place(at(way, d), 0)
        return remote(own if d == 0 else dst, dst, c_zs.at[m, way, d], c_zr.at[m, way, d],
                      (gr, (z + 1 if way == 0 else z - 1) * inner + y, tp))

    def y_slot(d, way):
        return d + way * (nz - 1) if d else 0

    def y_copy(m, q, way, d):
        own, place = items[m]
        zz = at(way, d)
        src = own if d == 0 else place(zz, 0)
        dst = place(zz, inner - q) if m == 0 else place(zz, 0)
        i = y_slot(d, way)
        return remote(src, dst, c_ys.at[m, q - 1, i], c_yr.at[m, q - 1, i],
                      (gr, z * inner + (y + q) % inner, tp))

    def pass_partner(m, part):
        if m:
            for p in range(1, n_gr):
                remote(part, part, g_send.at[m, p - 1], g_recv.at[m, p - 1],
                       ((gr + p) % n_gr, fs, tp)).start()

    def next_there(way):
        return (z < nz - 1) if way == 0 else (z > 0)

    def there(d, way):
        return (z - d >= 0) if way == 0 else (z + d < nz)

    @carried
    def gather_start(m):
        own, place = items[m]
        for way in (0, 1):
            pl.when(next_there(way))(lambda way=way: z_copy(m, way, 0).start())
        for q in range(1, inner):
            y_copy(m, q, 0, 0).start()
        if m:
            pltpu.make_async_copy(own, place(z, 0), c_own.at[m]).start()

    @carried
    def gather_own(m):
        own, place = items[m]
        pltpu.make_async_copy(own, place(z, 0), c_own.at[m]).wait()
        pass_partner(m, place(z, 0))

    @carried
    def gather_pass(m, d):
        for way in (0, 1):
            def act(way=way):
                part = items[m][1](at(way, d), 0)
                remote(part, part, c_zs.at[m, way, d - 1], c_zr.at[m, way, d - 1],
                       (gr, (z + 1 if way == 0 else z - 1) * inner + y, tp)).wait_recv()
                if d < nz - 1:
                    pl.when(next_there(way))(lambda: z_copy(m, way, d).start())
                for q in range(1, inner):
                    y_copy(m, q, way, d).start()
                pass_partner(m, part)
            pl.when(there(d, way))(act)

    places = [(0, 0)] + [(d, way) for d in range(1, nz) for way in (0, 1)]

    @carried
    def gather_y(m):
        for d, way in places:
            def act(d=d, way=way):
                for q in range(1, inner):
                    part = items[m][1](at(way, d), inner - q)
                    i = y_slot(d, way)
                    remote(part, part, c_ys.at[m, q - 1, i], c_yr.at[m, q - 1, i],
                           (gr, z * inner + (y + q) % inner, tp)).wait_recv()
                    pass_partner(m, part)
            if d == 0:
                act()
            else:
                pl.when(there(d, way))(act)

    @carried
    def gather_sent(m):
        for d, way in places:
            def act(d=d, way=way):
                for w in ((0, 1) if d == 0 else (way,)):
                    if d < nz - 1:
                        pl.when(next_there(w))(lambda w=w: z_copy(m, w, d).wait_send())
                for q in range(1, inner):
                    y_copy(m, q, way, d).wait_send()
            if d == 0:
                act()
            else:
                pl.when(there(d, way))(act)

    def partner_gathered(m, way):
        part = (X, GS, US, DS)[m]
        for p in range(1, n_gr):
            c = remote(part, part, g_send.at[m, p - 1], g_recv.at[m, p - 1],
                       ((gr + p) % n_gr, fs, tp))
            if way:
                pl.when(carrier)(c.wait_send)
            else:
                pl.when(gr == (n_gr - 1 + p) % n_gr)(c.wait_recv)

    per = depth // CT
    chunks = n_gr * per
    lanes = lax.broadcasted_iota(jnp.int32, (n_fs * R, cfg.extra), 1)
    dn = (((1,), (1,)), ((), ()))

    def gate_product(i, c):
        gg, n = (gr + i // per) % n_gr, i % per
        v = lax.dot_general(X[:, pl.ds(0, width)], W[0, gg, ds(n * CT, CT), :], dn,
                            preferred_element_type=F32)
        for r in range(inner):
            S[i * inner + r] = v[r * half:(r + 1) * half]
        return c

    def up_product(i, c):
        gg, n = (gr + i // per) % n_gr, i % per
        v = lax.dot_general(X[:, pl.ds(0, width)], W[1, gg, ds(n * CT, CT), :], dn,
                            preferred_element_type=F32)
        expert = gg * n_fs + fs
        pick = (lanes == expert) | (lanes == count + expert)
        weight = jnp.sum(jnp.where(pick, X[:, pl.ds(width, cfg.extra)].astype(F32), 0.0),
                         axis=1, keepdims=True)
        for r in range(inner):
            part = slice(r * half, (r + 1) * half)
            gate = S[i * inner + r]
            H[pl.ds(r * half, half), ds((gg * per + n) * CT, CT)] = (
                gate / (1.0 + jnp.exp(-gate)) * v[part] * weight[part]).astype(BF)
        return c

    pl.semaphore_wait(barrier, n_fs - 1 + n_tp - 1 + n_gr - 1)
    stops = max(1, nz - 1)
    size = -(-(n_fs - 1) // stops)
    parts = [(1 + k * size, min(n_fs, 1 + (k + 1) * size)) for k in range(stops)]
    gather_start(0)
    keep_own(0)
    each_other(lambda k: send(0, k), 1, 2)
    convert(1)
    keep_own(1)
    at_row = lax.broadcasted_iota(jnp.int32, (LG.shape[0], width), 0) + fs * LG.shape[0]
    at_col = lax.broadcasted_iota(jnp.int32, (LG.shape[0], width), 1)
    gain_rows = jnp.sum(jnp.where(at_row == at_col, gain_in[...], 0.0), axis=1, keepdims=True)
    LG[...] = (gs_in[...] * gain_rows).astype(BF)
    LU[...] = (us_in[...] * gain_rows).astype(BF)
    LD[...] = ds_in[...].astype(BF)
    convert(2)
    if nz > 1:
        gather_pass(0, 1)
    each_other(lambda k: send(0, k), 2, n_fs)
    for m in (1, 2, 3):
        gather_start(m)

    def second(s):
        landed(1, s)
        send(2, s)
    for k, part in enumerate(parts):
        each_other(lambda s: landed(0, s), *part)
        if k + 2 < nz - 1 or k + 2 == nz - 1 == 2:
            gather_pass(0, k + 2)
        each_other(lambda s: send(1, s), *part)
    if nz > 3:
        gather_pass(0, nz - 1)
    own_block(0).wait()
    share(0, 0)
    for m in range(2, 2 + DG):
        keep_own(m)
    shared_pass = [(lambda d=d: [gather_pass(m, d) for m in (1, 2, 3)]) for d in range(1, nz)]
    for m in (1, 2, 3):
        gather_own(m)
    for k, part in enumerate(parts):
        each_other(second, *part)
        if k == 0:
            for q in range(1, n_tp):
                x_landed(0, q)
                share(0, q)
        if k == max(0, stops - 2):
            gather_y(0)
            lax.fori_loop(0, per, gate_product, 0)
    for d in range(0, max(1, nz - 3)):
        shared_pass[d]()
    for m in range(3, 2 + DG):
        each_other(lambda k: send(m, k))
    own_block(1).wait()
    share(1, 0)
    for q in range(n_tp):
        shared_landed(0, q)
    lax.fori_loop(per, chunks, gate_product, 0)
    for q in range(1, n_tp):
        x_landed(1, q)
        share(1, q)

    def out_wide(m, g):
        return pltpu.make_async_copy(
            W.at[m, g, ds(tp * units, units), :], (gate_o, up_o)[m].at[g, 0], o_sem.at[m, g])

    def out_tall(g):
        return pltpu.make_async_copy(
            W.at[2, g, :, ds(tp * cols, cols)], down_o.at[g, 0], o_sem.at[2, g])

    for g in range(n_gr):
        out_wide(0, g).start()

    each = -(-(n_fs - 1) // chunks)

    def ahead(i, c):
        up_product(i, 0)
        each_other(lambda s: landed(2, s), 1 + i * each, jnp.minimum(n_fs, 1 + (i + 1) * each))
        return c
    lax.fori_loop(0, per, ahead, 0)
    for q in range(n_tp):
        shared_landed(1, q)
    for g in range(n_gr):
        out_wide(1, g).start()
    lax.fori_loop(per, chunks, ahead, 0)

    tiles = NT // n_tp
    each_group = tiles // DG
    group = n_tp * each_group

    def offset(i):
        late = jnp.where(i >= group, 1, 0) if DG > 1 else 0
        return (i // each_group + late) % n_tp

    def owner(i):
        return (tp + offset(i)) % n_tp

    def place_in(i):
        return i // group * each_group + i % each_group

    def y_out(i, r):
        return remote(PS.at[i, r - 1], YR.at[i, r - 1], y_send.at[i, r - 1], y_recv.at[i, r - 1],
                      (gr, z * inner + (y + r) % inner, tp))

    def produce(i, c):
        at_cols = ds((owner(i) * tiles + place_in(i)) * CT, CT)
        part = jnp.zeros((n_fs * R, CT), F32)
        for g in range(n_gr):
            part = part + jnp.dot(H[:, pl.ds(g * depth, depth)], W[2, g, :, at_cols],
                                  preferred_element_type=F32)
        S[i] = part[:half]
        for r in range(1, inner):
            PS[i, r - 1] = part[r * half:(r + 1) * half].astype(BF)

        @pl.when(i % each_group > 0)
        def _():
            for r in range(1, inner):
                y_out(i - 1, r).start()
        return c

    def tell(i):
        for r in range(1, inner):
            y_out(i, r).start()

    def make(a, u):
        m = 2 + a
        if u:
            x_landed(m, u)
        elif a == 0:
            own_block(m).wait()
        if u or a == 0:
            share(m, u)
        shared_landed(m, u)
        base = (a * n_tp + (n_tp - u - (1 if a else 0)) % n_tp) * each_group
        lax.fori_loop(base, base + each_group, produce, 0)
        tell(base + each_group - 1)

    def make_late(k, u):
        if k == 0:
            own_block(3).wait()
            share(3, 0)
        make(1, u)

    turn = [0] + [n_tp - u for u in range(1, n_tp)]
    for u in turn:
        make(0, u)
    for d in range(max(1, nz - 3), max(1, nz - 2)):
        shared_pass[d]()

    shared_outs = [pltpu.make_async_copy(a, b, o_sem.at[3 + i, 0])
                   for i, (a, b) in enumerate(((GS, gs_o), (US, us_o), (DS, ds_o)))]

    def sh_copy(q):
        return remote(SH.at[tp], SH.at[tp], sh_send.at[q - 1], sh_recv.at[q - 1],
                      (gr, fs, (tp + q) % n_tp))

    def shared_first():
        for m in (1, 2, 3):
            partner_gathered(m, 0)
        sg = jnp.dot(LN[...], GS[...], preferred_element_type=F32)
        su = jnp.dot(LN[...], US[...], preferred_element_type=F32)
        SH[tp] = (sg / (1.0 + jnp.exp(-sg)) * su).astype(BF)
        for c in shared_outs:
            c.start()
        for q in range(1, n_tp):
            sh_copy(q).start()

    def shared_rest():
        for q in range(1, n_tp):
            part = SH.at[(tp + n_tp - q) % n_tp]
            remote(part, part, sh_send.at[q - 1], sh_recv.at[q - 1], (gr, fs, (tp + q) % n_tp)).wait_recv()
        total = jnp.zeros((n_tp * R, cols), F32)
        su_n = GS.shape[1]
        for t in range(n_tp):
            total = total + jnp.dot(SH[t], DS[pl.ds(t * su_n, su_n), :], preferred_element_type=F32)
        SO[...] = total

    def z_move(way, i, lo, size, to):
        return remote(ZS.at[way, i, pl.ds(lo, size), :], ZR.at[way, i, pl.ds(lo, size), :],
                      z_send.at[way, i], z_recv.at[way, i], (gr, to * inner + y, tp))

    def upward(i, h):
        lo, size = (h + 1) * R, (nz - 1 - h) * R
        if h > 0:
            z_move(0, i, h * R, (nz - h) * R, z + 1).wait_recv()
            S[i, pl.ds(h * R, R), :] = S[i, pl.ds(h * R, R), :] + ZR[0, i, pl.ds(h * R, R), :].astype(F32)
            ZS[0, i, pl.ds(lo, size), :] = (
                S[i, pl.ds(lo, size), :] + ZR[0, i, pl.ds(lo, size), :].astype(F32)).astype(BF)
        else:
            ZS[0, i, pl.ds(lo, size), :] = S[i, pl.ds(lo, size), :].astype(BF)
        z_move(0, i, lo, size, z + 1).start()

    def downward(i, h):
        zz = nz - 1 - h
        size = zz * R
        if h > 0:
            z_move(1, i, 0, size + R, z - 1).wait_recv()
            S[i, pl.ds(size, R), :] = S[i, pl.ds(size, R), :] + ZR[1, i, pl.ds(size, R), :].astype(F32)
            ZS[1, i, pl.ds(0, size), :] = (
                S[i, pl.ds(0, size), :] + ZR[1, i, pl.ds(0, size), :].astype(F32)).astype(BF)
        else:
            ZS[1, i, pl.ds(0, size), :] = S[i, pl.ds(0, size), :].astype(BF)
        z_move(1, i, 0, size, z - 1).start()

    chain = NT - cfg.DT

    def straight(i, to):
        return remote(ZS.at[0, i, pl.ds(to * R, R), :], ZD.at[i - chain, z],
                      d_send.at[i - chain, to], d_recv.at[i - chain, z], (gr, to * inner + y, tp))

    def spread(i):
        ZS[0, i] = S[i].astype(BF)
        for to in range(nz):
            pl.when(z != to)(lambda to=to: straight(i, to).start())

    def gather_straight(i):
        for src in range(nz):
            @pl.when(z != src)
            def _(src=src):
                part = ZD.at[i - chain, src]
                remote(part, part, d_send.at[i - chain, src], d_recv.at[i - chain, src],
                       (gr, src * inner + y, tp)).wait_recv()
                S[i, ds(z * R, R), :] = S[i, ds(z * R, R), :] + ZD[i - chain, src].astype(F32)

    def f_copy(i):
        return remote(FS.at[i], FR.at[tp, place_in(i)], f_send.at[i], f_recv.at[tp, place_in(i)],
                      (gr, fs, owner(i)))

    def is_mine(i):
        return offset(i) == 0

    def end_chain(i):
        if nz > 1:
            last = (nz - 1) * R

            @pl.when(z == nz - 1)
            def _():
                z_move(0, i, last, R, z - 1).wait_recv()
                S[i, pl.ds(last, R), :] = S[i, pl.ds(last, R), :] + ZR[0, i, pl.ds(last, R), :].astype(F32)

            @pl.when(z == 0)
            def _():
                z_move(1, i, 0, R, z + 1).wait_recv()
                S[i, pl.ds(0, R), :] = S[i, pl.ds(0, R), :] + ZR[1, i, pl.ds(0, R), :].astype(F32)

    def finish(i):
        done = S[i, ds(z * R, R), :]

        @pl.when(is_mine(i))
        def _():
            at_cols = ds(place_in(i) * CT, CT)
            RO[:, at_cols] = done

        @pl.when(jnp.logical_not(is_mine(i)))
        def _():
            FS[i] = done.astype(BF)
            f_copy(i).start()

    turns = 3 if DG > 1 else 0
    some = -(-(n_fs - 1) // 3)

    def advance(j, c):
        if DG > 1:
            @pl.when(j < turns)
            def _():
                each_other(lambda s: landed(3, s), jnp.minimum(n_fs, 1 + j * some),
                           jnp.minimum(n_fs, 1 + (j + 1) * some))
            for k, u in enumerate(turn[1:] + turn[:1]):
                pl.when(j == turns + k)(lambda k=k, u=u: make_late(k, u))
        for d in range(max(1, nz - 2), nz - 1):
            pl.when(j == 1)(lambda d=d: [None, shared_pass[d]()][0])

        @pl.when(j < NT)
        def _():
            for r in range(1, inner):
                part = YR.at[j, r - 1]
                remote(part, part, y_send.at[j, r - 1], y_recv.at[j, r - 1],
                       (gr, z * inner + (y + r) % inner, tp)).wait_recv()
            S[j] = S[j] + sum([YR[j, r - 1].astype(F32) for r in range(1, inner)], 0.0)
        pl.when((j >= chain) & (j < NT))(lambda: spread(j))

        @pl.when(j == NT - 1)
        def _():
            for m in (1, 2, 3):
                gather_y(m)
        pl.when(j == NT)(shared_first)
        for h in range(nz - 1):
            i = j - h

            @pl.when((i >= 0) & (i < chain))
            def _(i=i, h=h):
                pl.when(z == h)(lambda: upward(i, h))
                pl.when(z == nz - 1 - h)(lambda: downward(i, h))
        i = j - (nz - 1)

        @pl.when((i >= 0) & (i < chain))
        def _():
            end_chain(i)
            finish(i)

        @pl.when((j > chain) & (j <= NT))
        def _():
            gather_straight(j - 1)
            finish(j - 1)
        return c
    lax.fori_loop(0, max(NT + 1, chain + nz - 1), advance, 0)
    for g in range(n_gr):
        out_tall(g).start()

    shared_rest()
    mixed_o[tp] = (RO[...] + SO[ds(tp * R, R), :]).astype(BF)

    def arrive(i, c):
        for q in range(1, n_tp):
            t = (tp + n_tp - q) % n_tp
            part = FR.at[t, i]
            remote(part, part, f_send.at[0], f_recv.at[t, i], (gr, fs, t)).wait_recv()
            at_cols = ds(i * CT, CT)
            mixed_o[t, :, at_cols] = (FR[t, i].astype(F32) + SO[ds(t * R, R), at_cols]).astype(BF)
        return c
    lax.fori_loop(0, tiles, arrive, 0)

    for m in range(2 + DG):
        lo, size_m = span(m)
        part = LB.at[min(m, 2), pl.ds(0, n_fs - 1), :, pl.ds(lo, size_m)]
        remote(part, part, b_send.at[m], b_send.at[m], (gr, fs, (tp + 1) % n_tp)).wait_send()
        for q in range(1, n_tp):
            part = region(m, gr, tp)
            remote(part, part, x_send.at[m, q - 1], x_recv.at[m, q - 1],
                   (gr, fs, (tp + q) % n_tp)).wait_send()
        for q in range(n_tp):
            for p in range(1, n_gr):
                partner(m, gr, q, p).wait_send()
    for m in range(4):
        gather_sent(m)
        if m:
            partner_gathered(m, 1)
    for q in range(1, n_tp):
        sh_copy(q).wait_send()

    def drain(i, c):
        for r in range(1, inner):
            y_out(i, r).wait_send()
        @pl.when(i < chain)
        def _():
            for h in range(nz - 1):
                pl.when(z == h)(lambda h=h: z_move(0, i, (h + 1) * R, (nz - 1 - h) * R, z + 1).wait_send())
                pl.when(z == nz - 1 - h)(lambda h=h: z_move(1, i, 0, (nz - 1 - h) * R, z - 1).wait_send())

        @pl.when(i >= chain)
        def _():
            for to in range(nz):
                pl.when(z != to)(lambda to=to: straight(i, to).wait_send())
        pl.when(jnp.logical_not(is_mine(i)))(lambda: f_copy(i).wait_send())
        return c
    lax.fori_loop(0, NT, drain, 0)
    for g in range(n_gr):
        out_tall(g).wait()
        for m in (0, 1):
            out_wide(m, g).wait()
    for c in shared_outs:
        c.wait()


class Config:
    pass


def on_device(tokens, routes, route_weight, norm_gain, gate_experts, up_experts, down_experts,
              gate_shared, up_shared, down_shared):
    dims = (lax.axis_size("gr"), lax.axis_size("fs"), lax.axis_size("tp"))
    n_gr, n_fs, n_tp = dims
    per_group, rows, cols = gate_experts.shape[1:]
    count = per_group * n_gr
    assert per_group == n_fs
    tok_count, top = routes.shape
    width = tokens.shape[1]
    depth = rows * n_fs
    units = depth // n_tp

    cfg = Config()
    cfg.dims = dims
    cfg.inner = inner = 2 if n_fs % 2 == 0 else 1
    cfg.nz = nz = n_fs // inner
    part = tok_count // n_tp
    cfg.R = R = -(-part // 16) * 16
    cfg.CT = CT = min(256, cols, depth)
    cfg.NT = NT = width // CT
    tiles = NT // n_tp
    cfg.DG = DG = 2 if tiles % 2 == 0 and tiles > 1 else 1
    cfg.DT = 2
    cfg.extra = extra = -(-2 * count // 128) * 128
    chunks = n_gr * depth // CT

    def in_parts(a):
        if R == part:
            return a
        a = jnp.pad(a.reshape(n_tp, part, a.shape[-1]), ((0, 0), (0, R - part), (0, 0)))
        return a.reshape(n_tp * R, a.shape[-1])

    gs, us, dsh = gate_shared, up_shared, down_shared
    sds = jax.ShapeDtypeStruct
    outs = (
        sds((n_tp, R, cols), BF),
        sds((n_gr, 1, units, width), BF),
        sds((n_gr, 1, units, width), BF),
        sds((n_gr, 1, depth, cols), BF),
        sds((n_fs * gs.shape[0], gs.shape[1]), BF),
        sds((n_fs * us.shape[0], us.shape[1]), BF),
        sds((n_fs * dsh.shape[0], dsh.shape[1]), BF),
    )
    V, DMA = pltpu.VMEM, pltpu.SemaphoreType.DMA
    q, p, r = max(1, n_tp - 1), max(1, n_gr - 1), max(1, inner - 1)
    M = 2 + DG
    scratch = [
        V((n_fs * R, width + extra), BF),
        V((3, n_gr, depth, width), BF),
        V((n_fs * R, n_gr * depth), BF),
        V(outs[4].shape, BF), V(outs[5].shape, BF), V(outs[6].shape, BF),
        V((n_tp, n_tp * R, gs.shape[1]), BF),
        V((n_tp * R, cols), F32),
        V((NT, r, nz * R, CT), BF), V((NT, r, nz * R, CT), BF),
        V((max(NT, chunks * inner), nz * R, CT), F32),
        V((2, NT, nz * R, CT), BF), V((2, NT, nz * R, CT), BF),
        V((cfg.DT, nz, R, CT), BF), V((NT, R, CT), BF), V((n_tp, tiles, R, CT), BF), V((R, cols), F32),
        V((2, n_fs, rows, cols), F32), V((3, n_fs, rows, cols), BF),
        V(gs.shape, BF), V(us.shape, BF), V(dsh.shape, BF),
        V((n_tp * R, width), BF),
        DMA((3,)),
        DMA((M,)), DMA((M, n_fs)), DMA((M,)), DMA((M, q)), DMA((M, q)),
        DMA((M, n_tp, p)), DMA((M, n_tp, p)),
        DMA((4, 2, nz)), DMA((4, 2, nz)), DMA((4, r, 2 * nz - 1)), DMA((4, r, 2 * nz - 1)),
        DMA((4,)), DMA((4, p)), DMA((4, p)),
        DMA((q,)), DMA((q,)), DMA((NT, r)), DMA((NT, r)), DMA((2, NT)), DMA((2, NT)),
        DMA((cfg.DT, nz)), DMA((cfg.DT, nz)),
        DMA((NT,)), DMA((n_tp, tiles)), DMA((6, n_gr)),
    ]
    anyw = pl.BlockSpec(memory_space=pl.ANY)
    vmem = pl.BlockSpec(memory_space=pltpu.VMEM)
    held = pl.pallas_call(
        functools.partial(whole, cfg),
        out_shape=tuple(V(o.shape, o.dtype) for o in outs),
        in_specs=[vmem] * 4 + [anyw] * 3 + [vmem] * 3,
        out_specs=(vmem,) * 7,
        scratch_shapes=scratch,
        compiler_params=pltpu.CompilerParams(
            collective_id=1, has_side_effects=True, vmem_limit_bytes=48 << 20),
        cost_estimate=pl.CostEstimate(flops=0, bytes_accessed=200 << 20, transcendentals=0),
    )(in_parts(tokens), in_parts(routes), in_parts(route_weight), norm_gain.reshape(1, width),
      gate_experts[0], up_experts[0], down_experts[0], gs, us, dsh)
    mixed, gate_w, up_w, down_w, gs_w, us_w, ds_w = pl.pallas_call(
        put,
        out_shape=outs,
        in_specs=[vmem] * 7,
        out_specs=(anyw,) * 7,
        scratch_shapes=[DMA((7,))],
        compiler_params=pltpu.CompilerParams(vmem_limit_bytes=1 << 20),
        cost_estimate=pl.CostEstimate(flops=0, bytes_accessed=20 << 20, transcendentals=0),
    )(*held)
    mixed = mixed[:, :part].reshape(tok_count, cols)
    return (mixed, gate_w, up_w, down_w, gs_w, us_w, ds_w)


def put(*refs):
    sems = refs[-1]
    copies = [pltpu.make_async_copy(a, b, sems.at[i]) for i, (a, b) in enumerate(zip(refs[:7], refs[7:14]))]
    for c in copies:
        c.start()
    for c in copies:
        c.wait()


def solution(mesh):
    return jax.shard_map(
        on_device,
        mesh=mesh,
        in_specs=(
            P(("gr", "fs"), None),
            P(("gr", "fs"), None),
            P(("gr", "fs"), None),
            P(),
            P("gr", None, "fs", "tp"),
            P("gr", None, "fs", "tp"),
            P("gr", None, "fs", "tp"),
            P("fs", "tp"),
            P("fs", "tp"),
            P("fs", "tp"),
        ),
        out_specs=(
            P(("gr", "fs"), "tp"),
            P(None, "fs", "tp", None),
            P(None, "fs", "tp", None),
            P(None, "fs", None, "tp"),
            P(None, "tp"),
            P(None, "tp"),
            P(None, "tp"),
        ),
        check_vma=False,
    )
```

```python
import functools

import jax
import jax.numpy as jnp
from jax import lax
from jax.experimental import pallas as pl
from jax.experimental.pallas import tpu as pltpu
from jax.sharding import PartitionSpec as P

EPS = 1e-06
MESH = pl.DeviceIdType.MESH
BF = jnp.bfloat16
F32 = jnp.float32


def whole(cfg, tok_in, route_in, weight_in, gain_in, gate_in, up_in, down_in, gs_in, us_in, ds_in,
          mixed_o, gate_o, up_o, down_o, gs_o, us_o, ds_o,
          X, W, H, GS, US, DS, SH, SO, PS, YR, S, ZS, ZR, ZD, FS, FR, RO, ST, LB, LG, LU, LD, LN,
          st_sem, b_send, b_recv, b_own, x_send, x_recv, p_send, p_recv,
          c_zs, c_zr, c_ys, c_yr, c_own, g_send, g_recv,
          sh_send, sh_recv, y_send, y_recv, z_send, z_recv, d_send, d_recv, f_send, f_recv, o_sem):
    n_gr, n_fs, n_tp = cfg.dims
    inner, nz, R, NT, CT, DG = cfg.inner, cfg.nz, cfg.R, cfg.NT, cfg.CT, cfg.DG
    gr, fs, tp = lax.axis_index("gr"), lax.axis_index("fs"), lax.axis_index("tp")
    z, y = fs // inner, fs % inner
    rows, cols = gate_in.shape[1], gate_in.shape[2]
    width = cols * n_tp
    depth = rows * n_fs
    units = depth // n_tp
    count = n_gr * n_fs
    half = nz * R

    def ds(start, size):
        if isinstance(start, int):
            return pl.ds(start, size)
        return pl.ds(pl.multiple_of(start * 1, size), size)

    def remote(src, dst, s, r, to):
        return pltpu.make_async_remote_copy(
            src_ref=src, dst_ref=dst, send_sem=s, recv_sem=r, device_id=to, device_id_type=MESH)

    barrier = pltpu.get_barrier_semaphore()

    def greet(d, c):
        pl.semaphore_signal(barrier, inc=1, device_id=(gr, (fs + d) % n_fs, tp), device_id_type=MESH)
        return c
    lax.fori_loop(1, n_fs, greet, 0)
    for q in range(1, n_tp):
        pl.semaphore_signal(barrier, inc=1, device_id=(gr, fs, (tp + q) % n_tp), device_id_type=MESH)
    for p in range(1, n_gr):
        pl.semaphore_signal(barrier, inc=1, device_id=((gr + p) % n_gr, fs, tp), device_id_type=MESH)

    def stage(m):
        return pltpu.make_async_copy((gate_in, up_in, down_in)[m], ST.at[m % 2], st_sem.at[m])
    stage(0).start()
    stage(1).start()

    def normalize(i, c):
        at_rows = ds(i * 16, 16)
        v = tok_in[at_rows, :].astype(F32)
        v = v * lax.rsqrt(jnp.mean(v * v, axis=-1, keepdims=True) + EPS)
        LN[at_rows, :] = v.astype(BF)
        return c
    lax.fori_loop(0, n_tp * R // 16, normalize, 0)
    mine = ds(tp * R, R)
    X[ds(z * R, R), pl.ds(0, width)] = LN[mine, :]
    own = (lax.broadcasted_iota(jnp.int32, (R, n_tp * R), 0) + tp * R
           == lax.broadcasted_iota(jnp.int32, (R, n_tp * R), 1))
    lane = lax.broadcasted_iota(jnp.int32, (R, cfg.extra), 1).astype(F32)
    tail = jnp.zeros((R, cfg.extra), F32)
    for j in range(route_in.shape[0]):
        e = jnp.sum(jnp.where(own, route_in[j:j + 1, :].astype(F32), 0.0), axis=1, keepdims=True)
        w = jnp.sum(jnp.where(own, weight_in[j:j + 1, :], 0.0), axis=1, keepdims=True)
        high = w.astype(BF).astype(F32)
        tail = tail + jnp.where(lane == e, high, 0.0) + jnp.where(lane == e + count, w - high, 0.0)
    X[ds(z * R, R), pl.ds(width, cfg.extra)] = tail.astype(BF)

    gain = gain_in[:, ds(tp * cols, cols)]

    def convert(m):
        stage(m).wait()

        def one(k, c):
            v = ST[m % 2, k]
            LB[m, k] = (v * gain if m < 2 else v).astype(BF)
            return c
        lax.fori_loop(0, n_fs, one, 0)
    convert(0)
    stage(2).start()

    gw = cols // DG

    def span(m):
        return (0, cols) if m < 2 else ((m - 2) * gw, gw)

    def block(m, s, t):
        lo, size = span(m)
        return W.at[min(m, 2), gr, ds(s * rows, rows), pl.ds(pl.multiple_of(t * cols + lo, size), size)]

    def region(m, g, t):
        lo, size = span(m)
        return W.at[min(m, 2), g, :, pl.ds(pl.multiple_of(t * cols + lo, size), size)]

    def local(m, k):
        lo, size = span(m)
        return LB.at[min(m, 2), k, :, pl.ds(lo, size)]

    def to_expert(m, k):
        return remote(local(m, k), block(m, fs, tp), b_send.at[m], b_recv.at[m, fs], (gr, k, tp))

    def own_block(m):
        return pltpu.make_async_copy(local(m, fs), block(m, fs, tp), b_own.at[m])

    def each_other(act, lo=1, hi=n_fs):
        def step(d, c):
            pl.when(fs + d < n_fs)(lambda: act(fs + d))
            pl.when(fs - d >= 0)(lambda: act(fs - d))
            return c
        lax.fori_loop(lo, hi, step, 0)

    def across(m, src, s):
        for q in range(1, n_tp):
            remote(src, block(m, s, tp), x_send.at[m, q - 1], x_recv.at[m, q - 1],
                   (gr, fs, (tp + q) % n_tp)).start()

    def keep_own(m):
        own_block(m).start()
        across(m, local(m, fs), fs)

    def send(m, k):
        to_expert(m, k).start()

    def landed(m, s):
        part = block(m, s, tp)
        remote(part, part, b_recv.at[m, s], b_recv.at[m, s], (gr, s, tp)).wait_recv()
        across(m, part, s)

    def partner(m, g, q, p):
        part = region(m, g, (tp + n_tp - q) % n_tp)
        return remote(part, part, p_send.at[m, q, p - 1], p_recv.at[m, q, p - 1],
                      ((gr + p) % n_gr, fs, tp))

    def share(m, q):
        for p in range(1, n_gr):
            partner(m, gr, q, p).start()

    def shared_landed(m, q):
        for p in range(1, n_gr):
            partner(m, (gr + n_gr - p) % n_gr, q, p).wait_recv()

    def x_landed(m, q):
        part = region(m, gr, (tp + n_tp - q) % n_tp)
        remote(part, part, x_send.at[m, q - 1], x_recv.at[m, q - 1],
               (gr, fs, (tp + q) % n_tp)).wait_recv()

    def token_place(zz, yr):
        return X.at[ds((yr * nz + zz) * R, R), :]

    def shared_item(src, dst):
        size = src.shape[0]

        def place(zz, yr):
            return dst.at[ds((zz * inner + (y + yr) % inner) * size, size), :]
        return (src, place)
    items = ((token_place(z, 0), token_place),) + tuple(
        shared_item(s, d) for s, d in zip((LG, LU, LD), (GS, US, DS)))
    carrier = gr == n_gr - 1

    def carried(f):
        def run(m, *rest):
            if m:
                pl.when(carrier)(lambda: f(m, *rest))
            else:
                f(m, *rest)
        return run

    def at(way, d):
        return z - d if way == 0 else z + d

    def z_copy(m, way, d):
        own, place = items[m]
        dst = place(at(way, d), 0)
        return remote(own if d == 0 else dst, dst, c_zs.at[m, way, d], c_zr.at[m, way, d],
                      (gr, (z + 1 if way == 0 else z - 1) * inner + y, tp))

    def y_slot(d, way):
        return d + way * (nz - 1) if d else 0

    def y_copy(m, q, way, d):
        own, place = items[m]
        zz = at(way, d)
        src = own if d == 0 else place(zz, 0)
        dst = place(zz, inner - q) if m == 0 else place(zz, 0)
        i = y_slot(d, way)
        return remote(src, dst, c_ys.at[m, q - 1, i], c_yr.at[m, q - 1, i],
                      (gr, z * inner + (y + q) % inner, tp))

    def pass_partner(m, part):
        if m:
            for p in range(1, n_gr):
                remote(part, part, g_send.at[m, p - 1], g_recv.at[m, p - 1],
                       ((gr + p) % n_gr, fs, tp)).start()

    def next_there(way):
        return (z < nz - 1) if way == 0 else (z > 0)

    def there(d, way):
        return (z - d >= 0) if way == 0 else (z + d < nz)

    @carried
    def gather_start(m):
        own, place = items[m]
        for way in (0, 1):
            pl.when(next_there(way))(lambda way=way: z_copy(m, way, 0).start())
        for q in range(1, inner):
            y_copy(m, q, 0, 0).start()
        if m:
            pltpu.make_async_copy(own, place(z, 0), c_own.at[m]).start()

    @carried
    def gather_own(m):
        own, place = items[m]
        pltpu.make_async_copy(own, place(z, 0), c_own.at[m]).wait()
        pass_partner(m, place(z, 0))

    @carried
    def gather_pass(m, d):
        for way in (0, 1):
            def act(way=way):
                part = items[m][1](at(way, d), 0)
                remote(part, part, c_zs.at[m, way, d - 1], c_zr.at[m, way, d - 1],
                       (gr, (z + 1 if way == 0 else z - 1) * inner + y, tp)).wait_recv()
                if d < nz - 1:
                    pl.when(next_there(way))(lambda: z_copy(m, way, d).start())
                for q in range(1, inner):
                    y_copy(m, q, way, d).start()
                pass_partner(m, part)
            pl.when(there(d, way))(act)

    places = [(0, 0)] + [(d, way) for d in range(1, nz) for way in (0, 1)]

    @carried
    def gather_y(m):
        for d, way in places:
            def act(d=d, way=way):
                for q in range(1, inner):
                    part = items[m][1](at(way, d), inner - q)
                    i = y_slot(d, way)
                    remote(part, part, c_ys.at[m, q - 1, i], c_yr.at[m, q - 1, i],
                           (gr, z * inner + (y + q) % inner, tp)).wait_recv()
                    pass_partner(m, part)
            if d == 0:
                act()
            else:
                pl.when(there(d, way))(act)

    @carried
    def gather_sent(m):
        for d, way in places:
            def act(d=d, way=way):
                for w in ((0, 1) if d == 0 else (way,)):
                    if d < nz - 1:
                        pl.when(next_there(w))(lambda w=w: z_copy(m, w, d).wait_send())
                for q in range(1, inner):
                    y_copy(m, q, way, d).wait_send()
            if d == 0:
                act()
            else:
                pl.when(there(d, way))(act)

    def partner_gathered(m, way):
        part = (X, GS, US, DS)[m]
        for p in range(1, n_gr):
            c = remote(part, part, g_send.at[m, p - 1], g_recv.at[m, p - 1],
                       ((gr + p) % n_gr, fs, tp))
            if way:
                pl.when(carrier)(c.wait_send)
            else:
                pl.when(gr == (n_gr - 1 + p) % n_gr)(c.wait_recv)

    per = depth // CT
    chunks = n_gr * per
    lanes = lax.broadcasted_iota(jnp.int32, (n_fs * R, cfg.extra), 1)
    dn = (((1,), (1,)), ((), ()))

    def gate_product(i, c):
        gg, n = (gr + i // per) % n_gr, i % per
        v = lax.dot_general(X[:, pl.ds(0, width)], W[0, gg, ds(n * CT, CT), :], dn,
                            preferred_element_type=F32)
        for r in range(inner):
            S[i * inner + r] = v[r * half:(r + 1) * half]
        return c

    def up_product(i, c):
        gg, n = (gr + i // per) % n_gr, i % per
        v = lax.dot_general(X[:, pl.ds(0, width)], W[1, gg, ds(n * CT, CT), :], dn,
                            preferred_element_type=F32)
        expert = gg * n_fs + fs
        pick = (lanes == expert) | (lanes == count + expert)
        weight = jnp.sum(jnp.where(pick, X[:, pl.ds(width, cfg.extra)].astype(F32), 0.0),
                         axis=1, keepdims=True)
        for r in range(inner):
            part = slice(r * half, (r + 1) * half)
            gate = S[i * inner + r]
            H[pl.ds(r * half, half), ds((gg * per + n) * CT, CT)] = (
                gate / (1.0 + jnp.exp(-gate)) * v[part] * weight[part]).astype(BF)
        return c

    pl.semaphore_wait(barrier, n_fs - 1 + n_tp - 1 + n_gr - 1)
    stops = max(1, nz - 1)
    size = -(-(n_fs - 1) // stops)
    parts = [(1 + k * size, min(n_fs, 1 + (k + 1) * size)) for k in range(stops)]
    gather_start(0)
    keep_own(0)
    each_other(lambda k: send(0, k), 1, 2)
    convert(1)
    keep_own(1)
    at_row = lax.broadcasted_iota(jnp.int32, (LG.shape[0], width), 0) + fs * LG.shape[0]
    at_col = lax.broadcasted_iota(jnp.int32, (LG.shape[0], width), 1)
    gain_rows = jnp.sum(jnp.where(at_row == at_col, gain_in[...], 0.0), axis=1, keepdims=True)
    LG[...] = (gs_in[...] * gain_rows).astype(BF)
    LU[...] = (us_in[...] * gain_rows).astype(BF)
    LD[...] = ds_in[...].astype(BF)
    convert(2)
    if nz > 1:
        gather_pass(0, 1)
    each_other(lambda k: send(0, k), 2, n_fs)
    for m in (1, 2, 3):
        gather_start(m)

    def second(s):
        landed(1, s)
        send(2, s)
    for k, part in enumerate(parts):
        each_other(lambda s: landed(0, s), *part)
        if k + 2 < nz - 1 or k + 2 == nz - 1 == 2:
            gather_pass(0, k + 2)
        each_other(lambda s: send(1, s), *part)
    if nz > 3:
        gather_pass(0, nz - 1)
    own_block(0).wait()
    share(0, 0)
    for m in range(2, 2 + DG):
        keep_own(m)
    shared_pass = [(lambda d=d: [gather_pass(m, d) for m in (1, 2, 3)]) for d in range(1, nz)]
    for m in (1, 2, 3):
        gather_own(m)
    for k, part in enumerate(parts):
        each_other(second, *part)
        if k == 0:
            for q in range(1, n_tp):
                x_landed(0, q)
                share(0, q)
        if k == max(0, stops - 2):
            gather_y(0)
            lax.fori_loop(0, per, gate_product, 0)
    for d in range(0, max(1, nz - 3)):
        shared_pass[d]()
    for m in range(3, 2 + DG):
        each_other(lambda k: send(m, k))
    own_block(1).wait()
    share(1, 0)
    for q in range(n_tp):
        shared_landed(0, q)
    lax.fori_loop(per, chunks, gate_product, 0)
    for q in range(1, n_tp):
        x_landed(1, q)
        share(1, q)

    def out_wide(m, g):
        return pltpu.make_async_copy(
            W.at[m, g, ds(tp * units, units), :], (gate_o, up_o)[m].at[g, 0], o_sem.at[m, g])

    def out_tall(g):
        return pltpu.make_async_copy(
            W.at[2, g, :, ds(tp * cols, cols)], down_o.at[g, 0], o_sem.at[2, g])

    for g in range(n_gr):
        out_wide(0, g).start()

    each = -(-(n_fs - 1) // chunks)

    def ahead(i, c):
        up_product(i, 0)
        each_other(lambda s: landed(2, s), 1 + i * each, jnp.minimum(n_fs, 1 + (i + 1) * each))
        return c
    lax.fori_loop(0, per, ahead, 0)
    for q in range(n_tp):
        shared_landed(1, q)
    for g in range(n_gr):
        out_wide(1, g).start()
    lax.fori_loop(per, chunks, ahead, 0)

    tiles = NT // n_tp
    each_group = tiles // DG
    group = n_tp * each_group

    def offset(i):
        late = jnp.where(i >= group, 1, 0) if DG > 1 else 0
        return (i // each_group + late) % n_tp

    def owner(i):
        return (tp + offset(i)) % n_tp

    def place_in(i):
        return i // group * each_group + i % each_group

    def y_out(i, r):
        return remote(PS.at[i, r - 1], YR.at[i, r - 1], y_send.at[i, r - 1], y_recv.at[i, r - 1],
                      (gr, z * inner + (y + r) % inner, tp))

    def produce(i, c):
        at_cols = ds((owner(i) * tiles + place_in(i)) * CT, CT)
        part = jnp.zeros((n_fs * R, CT), F32)
        for g in range(n_gr):
            part = part + jnp.dot(H[:, pl.ds(g * depth, depth)], W[2, g, :, at_cols],
                                  preferred_element_type=F32)
        S[i] = part[:half]
        for r in range(1, inner):
            PS[i, r - 1] = part[r * half:(r + 1) * half].astype(BF)

        @pl.when(i % each_group > 0)
        def _():
            for r in range(1, inner):
                y_out(i - 1, r).start()
        return c

    def tell(i):
        for r in range(1, inner):
            y_out(i, r).start()

    def make(a, u):
        m = 2 + a
        if u:
            x_landed(m, u)
        elif a == 0:
            own_block(m).wait()
        if u or a == 0:
            share(m, u)
        shared_landed(m, u)
        base = (a * n_tp + (n_tp - u - (1 if a else 0)) % n_tp) * each_group
        lax.fori_loop(base, base + each_group, produce, 0)
        tell(base + each_group - 1)

    def make_late(k, u):
        if k == 0:
            own_block(3).wait()
            share(3, 0)
        make(1, u)

    turn = [0] + [n_tp - u for u in range(1, n_tp)]
    for u in turn:
        make(0, u)
    for d in range(max(1, nz - 3), max(1, nz - 2)):
        shared_pass[d]()

    shared_outs = [pltpu.make_async_copy(a, b, o_sem.at[3 + i, 0])
                   for i, (a, b) in enumerate(((GS, gs_o), (US, us_o), (DS, ds_o)))]

    def sh_copy(q):
        return remote(SH.at[tp], SH.at[tp], sh_send.at[q - 1], sh_recv.at[q - 1],
                      (gr, fs, (tp + q) % n_tp))

    def shared_first():
        for m in (1, 2, 3):
            partner_gathered(m, 0)
        sg = jnp.dot(LN[...], GS[...], preferred_element_type=F32)
        su = jnp.dot(LN[...], US[...], preferred_element_type=F32)
        SH[tp] = (sg / (1.0 + jnp.exp(-sg)) * su).astype(BF)
        for c in shared_outs:
            c.start()
        for q in range(1, n_tp):
            sh_copy(q).start()

    def shared_rest():
        for q in range(1, n_tp):
            part = SH.at[(tp + n_tp - q) % n_tp]
            remote(part, part, sh_send.at[q - 1], sh_recv.at[q - 1], (gr, fs, (tp + q) % n_tp)).wait_recv()
        total = jnp.zeros((n_tp * R, cols), F32)
        su_n = GS.shape[1]
        for t in range(n_tp):
            total = total + jnp.dot(SH[t], DS[pl.ds(t * su_n, su_n), :], preferred_element_type=F32)
        SO[...] = total

    def z_move(way, i, lo, size, to):
        return remote(ZS.at[way, i, pl.ds(lo, size), :], ZR.at[way, i, pl.ds(lo, size), :],
                      z_send.at[way, i], z_recv.at[way, i], (gr, to * inner + y, tp))

    def upward(i, h):
        lo, size = (h + 1) * R, (nz - 1 - h) * R
        if h > 0:
            z_move(0, i, h * R, (nz - h) * R, z + 1).wait_recv()
            S[i, pl.ds(h * R, R), :] = S[i, pl.ds(h * R, R), :] + ZR[0, i, pl.ds(h * R, R), :].astype(F32)
            ZS[0, i, pl.ds(lo, size), :] = (
                S[i, pl.ds(lo, size), :] + ZR[0, i, pl.ds(lo, size), :].astype(F32)).astype(BF)
        else:
            ZS[0, i, pl.ds(lo, size), :] = S[i, pl.ds(lo, size), :].astype(BF)
        z_move(0, i, lo, size, z + 1).start()

    def downward(i, h):
        zz = nz - 1 - h
        size = zz * R
        if h > 0:
            z_move(1, i, 0, size + R, z - 1).wait_recv()
            S[i, pl.ds(size, R), :] = S[i, pl.ds(size, R), :] + ZR[1, i, pl.ds(size, R), :].astype(F32)
            ZS[1, i, pl.ds(0, size), :] = (
                S[i, pl.ds(0, size), :] + ZR[1, i, pl.ds(0, size), :].astype(F32)).astype(BF)
        else:
            ZS[1, i, pl.ds(0, size), :] = S[i, pl.ds(0, size), :].astype(BF)
        z_move(1, i, 0, size, z - 1).start()

    chain = NT - cfg.DT

    def straight(i, to):
        return remote(ZS.at[0, i, pl.ds(to * R, R), :], ZD.at[i - chain, z],
                      d_send.at[i - chain, to], d_recv.at[i - chain, z], (gr, to * inner + y, tp))

    def spread(i):
        ZS[0, i] = S[i].astype(BF)
        for to in range(nz):
            pl.when(z != to)(lambda to=to: straight(i, to).start())

    def gather_straight(i):
        for src in range(nz):
            @pl.when(z != src)
            def _(src=src):
                part = ZD.at[i - chain, src]
                remote(part, part, d_send.at[i - chain, src], d_recv.at[i - chain, src],
                       (gr, src * inner + y, tp)).wait_recv()
                S[i, ds(z * R, R), :] = S[i, ds(z * R, R), :] + ZD[i - chain, src].astype(F32)

    def f_copy(i):
        return remote(FS.at[i], FR.at[tp, place_in(i)], f_send.at[i], f_recv.at[tp, place_in(i)],
                      (gr, fs, owner(i)))

    def is_mine(i):
        return offset(i) == 0

    def end_chain(i):
        if nz > 1:
            last = (nz - 1) * R

            @pl.when(z == nz - 1)
            def _():
                z_move(0, i, last, R, z - 1).wait_recv()
                S[i, pl.ds(last, R), :] = S[i, pl.ds(last, R), :] + ZR[0, i, pl.ds(last, R), :].astype(F32)

            @pl.when(z == 0)
            def _():
                z_move(1, i, 0, R, z + 1).wait_recv()
                S[i, pl.ds(0, R), :] = S[i, pl.ds(0, R), :] + ZR[1, i, pl.ds(0, R), :].astype(F32)

    def finish(i):
        done = S[i, ds(z * R, R), :]

        @pl.when(is_mine(i))
        def _():
            at_cols = ds(place_in(i) * CT, CT)
            RO[:, at_cols] = done

        @pl.when(jnp.logical_not(is_mine(i)))
        def _():
            FS[i] = done.astype(BF)
            f_copy(i).start()

    turns = 3 if DG > 1 else 0
    some = -(-(n_fs - 1) // 3)

    def advance(j, c):
        if DG > 1:
            @pl.when(j < turns)
            def _():
                each_other(lambda s: landed(3, s), jnp.minimum(n_fs, 1 + j * some),
                           jnp.minimum(n_fs, 1 + (j + 1) * some))
            for k, u in enumerate(turn[1:] + turn[:1]):
                pl.when(j == turns + k)(lambda k=k, u=u: make_late(k, u))
        for d in range(max(1, nz - 2), nz - 1):
            pl.when(j == 1)(lambda d=d: [None, shared_pass[d]()][0])

        @pl.when(j < NT)
        def _():
            for r in range(1, inner):
                part = YR.at[j, r - 1]
                remote(part, part, y_send.at[j, r - 1], y_recv.at[j, r - 1],
                       (gr, z * inner + (y + r) % inner, tp)).wait_recv()
            S[j] = S[j] + sum([YR[j, r - 1].astype(F32) for r in range(1, inner)], 0.0)
        pl.when((j >= chain) & (j < NT))(lambda: spread(j))

        @pl.when(j == NT - 1)
        def _():
            for m in (1, 2, 3):
                gather_y(m)
        pl.when(j == NT)(shared_first)
        for h in range(nz - 1):
            i = j - h

            @pl.when((i >= 0) & (i < chain))
            def _(i=i, h=h):
                pl.when(z == h)(lambda: upward(i, h))
                pl.when(z == nz - 1 - h)(lambda: downward(i, h))
        i = j - (nz - 1)

        @pl.when((i >= 0) & (i < chain))
        def _():
            end_chain(i)
            finish(i)

        @pl.when((j > chain) & (j <= NT))
        def _():
            gather_straight(j - 1)
            finish(j - 1)
        return c
    lax.fori_loop(0, max(NT + 1, chain + nz - 1), advance, 0)
    for g in range(n_gr):
        out_tall(g).start()

    shared_rest()
    mixed_o[tp] = (RO[...] + SO[ds(tp * R, R), :]).astype(BF)

    def arrive(i, c):
        for q in range(1, n_tp):
            t = (tp + n_tp - q) % n_tp
            part = FR.at[t, i]
            remote(part, part, f_send.at[0], f_recv.at[t, i], (gr, fs, t)).wait_recv()
            at_cols = ds(i * CT, CT)
            mixed_o[t, :, at_cols] = (FR[t, i].astype(F32) + SO[ds(t * R, R), at_cols]).astype(BF)
        return c
    lax.fori_loop(0, tiles, arrive, 0)

    for m in range(2 + DG):
        lo, size_m = span(m)
        part = LB.at[min(m, 2), pl.ds(0, n_fs - 1), :, pl.ds(lo, size_m)]
        remote(part, part, b_send.at[m], b_send.at[m], (gr, fs, (tp + 1) % n_tp)).wait_send()
        for q in range(1, n_tp):
            part = region(m, gr, tp)
            remote(part, part, x_send.at[m, q - 1], x_recv.at[m, q - 1],
                   (gr, fs, (tp + q) % n_tp)).wait_send()
        for q in range(n_tp):
            for p in range(1, n_gr):
                partner(m, gr, q, p).wait_send()
    for m in range(4):
        gather_sent(m)
        if m:
            partner_gathered(m, 1)
    for q in range(1, n_tp):
        sh_copy(q).wait_send()

    def drain(i, c):
        for r in range(1, inner):
            y_out(i, r).wait_send()
        @pl.when(i < chain)
        def _():
            for h in range(nz - 1):
                pl.when(z == h)(lambda h=h: z_move(0, i, (h + 1) * R, (nz - 1 - h) * R, z + 1).wait_send())
                pl.when(z == nz - 1 - h)(lambda h=h: z_move(1, i, 0, (nz - 1 - h) * R, z - 1).wait_send())

        @pl.when(i >= chain)
        def _():
            for to in range(nz):
                pl.when(z != to)(lambda to=to: straight(i, to).wait_send())
        pl.when(jnp.logical_not(is_mine(i)))(lambda: f_copy(i).wait_send())
        return c
    lax.fori_loop(0, NT, drain, 0)
    for g in range(n_gr):
        out_tall(g).wait()
        for m in (0, 1):
            out_wide(m, g).wait()
    for c in shared_outs:
        c.wait()


class Config:
    pass


def on_device(tokens, routes, route_weight, norm_gain, gate_experts, up_experts, down_experts,
              gate_shared, up_shared, down_shared):
    dims = (lax.axis_size("gr"), lax.axis_size("fs"), lax.axis_size("tp"))
    n_gr, n_fs, n_tp = dims
    per_group, rows, cols = gate_experts.shape[1:]
    count = per_group * n_gr
    assert per_group == n_fs
    tok_count, top = routes.shape
    width = tokens.shape[1]
    depth = rows * n_fs
    units = depth // n_tp

    cfg = Config()
    cfg.dims = dims
    cfg.inner = inner = 2 if n_fs % 2 == 0 else 1
    cfg.nz = nz = n_fs // inner
    part = tok_count // n_tp
    cfg.R = R = -(-part // 16) * 16
    cfg.CT = CT = min(256, cols, depth)
    cfg.NT = NT = width // CT
    tiles = NT // n_tp
    cfg.DG = DG = 2 if tiles % 2 == 0 and tiles > 1 else 1
    cfg.DT = max(2, NT // 2)
    cfg.extra = extra = -(-2 * count // 128) * 128
    chunks = n_gr * depth // CT

    def in_parts(a):
        if R == part:
            return a
        a = jnp.pad(a.reshape(n_tp, part, a.shape[-1]), ((0, 0), (0, R - part), (0, 0)))
        return a.reshape(n_tp * R, a.shape[-1])

    gs, us, dsh = gate_shared, up_shared, down_shared
    sds = jax.ShapeDtypeStruct
    outs = (
        sds((n_tp, R, cols), BF),
        sds((n_gr, 1, units, width), BF),
        sds((n_gr, 1, units, width), BF),
        sds((n_gr, 1, depth, cols), BF),
        sds((n_fs * gs.shape[0], gs.shape[1]), BF),
        sds((n_fs * us.shape[0], us.shape[1]), BF),
        sds((n_fs * dsh.shape[0], dsh.shape[1]), BF),
    )
    V, DMA = pltpu.VMEM, pltpu.SemaphoreType.DMA
    q, p, r = max(1, n_tp - 1), max(1, n_gr - 1), max(1, inner - 1)
    M = 2 + DG
    scratch = [
        V((n_fs * R, width + extra), BF),
        V((3, n_gr, depth, width), BF),
        V((n_fs * R, n_gr * depth), BF),
        V(outs[4].shape, BF), V(outs[5].shape, BF), V(outs[6].shape, BF),
        V((n_tp, n_tp * R, gs.shape[1]), BF),
        V((n_tp * R, cols), F32),
        V((NT, r, nz * R, CT), BF), V((NT, r, nz * R, CT), BF),
        V((max(NT, chunks * inner), nz * R, CT), F32),
        V((2, NT, nz * R, CT), BF), V((2, NT, nz * R, CT), BF),
        V((cfg.DT, nz, R, CT), BF), V((NT, R, CT), BF), V((n_tp, tiles, R, CT), BF), V((R, cols), F32),
        V((2, n_fs, rows, cols), F32), V((3, n_fs, rows, cols), BF),
        V(gs.shape, BF), V(us.shape, BF), V(dsh.shape, BF),
        V((n_tp * R, width), BF),
        DMA((3,)),
        DMA((M,)), DMA((M, n_fs)), DMA((M,)), DMA((M, q)), DMA((M, q)),
        DMA((M, n_tp, p)), DMA((M, n_tp, p)),
        DMA((4, 2, nz)), DMA((4, 2, nz)), DMA((4, r, 2 * nz - 1)), DMA((4, r, 2 * nz - 1)),
        DMA((4,)), DMA((4, p)), DMA((4, p)),
        DMA((q,)), DMA((q,)), DMA((NT, r)), DMA((NT, r)), DMA((2, NT)), DMA((2, NT)),
        DMA((cfg.DT, nz)), DMA((cfg.DT, nz)),
        DMA((NT,)), DMA((n_tp, tiles)), DMA((6, n_gr)),
    ]
    anyw = pl.BlockSpec(memory_space=pl.ANY)
    vmem = pl.BlockSpec(memory_space=pltpu.VMEM)
    held = pl.pallas_call(
        functools.partial(whole, cfg),
        out_shape=tuple(V(o.shape, o.dtype) for o in outs),
        in_specs=[vmem] * 4 + [anyw] * 3 + [vmem] * 3,
        out_specs=(vmem,) * 7,
        scratch_shapes=scratch,
        compiler_params=pltpu.CompilerParams(
            collective_id=1, has_side_effects=True, vmem_limit_bytes=48 << 20),
        cost_estimate=pl.CostEstimate(flops=0, bytes_accessed=200 << 20, transcendentals=0),
    )(in_parts(tokens), in_parts(routes).T, in_parts(route_weight).T, norm_gain.reshape(1, width),
      gate_experts[0], up_experts[0], down_experts[0], gs, us, dsh)
    mixed, gate_w, up_w, down_w, gs_w, us_w, ds_w = pl.pallas_call(
        put,
        out_shape=outs,
        in_specs=[vmem] * 7,
        out_specs=(anyw,) * 7,
        scratch_shapes=[DMA((7,))],
        compiler_params=pltpu.CompilerParams(vmem_limit_bytes=1 << 20),
        cost_estimate=pl.CostEstimate(flops=0, bytes_accessed=20 << 20, transcendentals=0),
    )(*held)
    mixed = mixed[:, :part].reshape(tok_count, cols)
    return (mixed, gate_w, up_w, down_w, gs_w, us_w, ds_w)


def put(*refs):
    sems = refs[-1]
    copies = [pltpu.make_async_copy(a, b, sems.at[i]) for i, (a, b) in enumerate(zip(refs[:7], refs[7:14]))]
    for c in copies:
        c.start()
    for c in copies:
        c.wait()


def solution(mesh):
    return jax.shard_map(
        on_device,
        mesh=mesh,
        in_specs=(
            P(("gr", "fs"), None),
            P(("gr", "fs"), None),
            P(("gr", "fs"), None),
            P(),
            P("gr", None, "fs", "tp"),
            P("gr", None, "fs", "tp"),
            P("gr", None, "fs", "tp"),
            P("fs", "tp"),
            P("fs", "tp"),
            P("fs", "tp"),
        ),
        out_specs=(
            P(("gr", "fs"), "tp"),
            P(None, "fs", "tp", None),
            P(None, "fs", "tp", None),
            P(None, "fs", None, "tp"),
            P(None, "tp"),
            P(None, "tp"),
            P(None, "tp"),
        ),
        check_vma=False,
    )
```
